512 devices in a mesh: ep: 32 (over z, x), tp: 16 (over y, core).
Axes of the slice: x: 4, y: 8, z: 8, core: 2. Of those that a mesh axis runs over, the one named last changes fastest.
Arguments:
- tokens: bfloat16 [256, 4096], P('ep', 'tp'), may hold values from -6 to 6
- norm_gain: float32 [4096], replicated, may hold values from 0.1 to 1.9
- route_experts: int32 [256, 2], P('ep'), may hold values from 0 to 63, all different within a row; in each aligned block of 8 rows (0 to 7, 8 to 15, ...) at most 2 rows name the same one
- route_logits: float32 [256, 2], P('ep'), may hold values from -4 to 4
- expert_gate: bfloat16 [64, 4096, 1024], P('ep', None, 'tp'), may hold values from -0.09375 to 0.09375
- expert_up: bfloat16 [64, 4096, 1024], P('ep', None, 'tp'), may hold values from -0.09375 to 0.09375
- expert_down: bfloat16 [64, 1024, 4096], P('ep', 'tp'), may hold values from -0.1875 to 0.1875
- dense_gate: bfloat16 [4096, 1024], P(None, 'tp'), may hold values from -0.09375 to 0.09375
- dense_up: bfloat16 [4096, 1024], P(None, 'tp'), may hold values from -0.09375 to 0.09375
- dense_down: bfloat16 [1024, 4096], P('tp'), may hold values from -0.1875 to 0.1875
- mix_weight: float32 [4096], replicated, may hold values from -0.09375 to 0.09375
- out_gain: float32 [4096], P('tp'), may hold values from 0.1 to 1.9
Outputs:
- result: bfloat16 [256, 4096], P('ep', 'tp')
The draws below stay inside these ranges and needn't reach their ends.
Inputs may be any that keep to these rules, and one draw needn't show every extreme that they name: `route_experts`: each row names 2 different experts; the 8 rows of one index of ep (aligned blocks) name any one expert at most 2 times, and some block names some expert exactly 2 times; every expert is named somewhere.
All inputs are finite; a program needn't handle non-finite values.
Results may differ from the reference program's by a relative error of at most 0.0025.
Values may be sent and summed in bfloat16 or wider, within the bound.
A program may use at most 64 MiB of HBM per device.

```python
import math
import jax
import jax.numpy as jnp
import numpy as np
from jax import lax

D = 4096
FFE = 1024
DENSE_FF = 1024
TOP = 2
CAP = 2
TOK_DEV = 8
EXPERTS = 64
TOKENS = 256
N_EP = 32


def levels(rng, dims, pieces, low, high):
    level = 1.0
    for dim, shards_of in pieces:
        draws = jax.random.uniform(jax.random.fold_in(jax.random.fold_in(rng, 6), dim), (shards_of,), jnp.float32, low / len(pieces), high / len(pieces))
        level = level * jnp.repeat(jnp.exp(draws), dims[dim] // shards_of).reshape((-1,) + (1,) * (len(dims) - 1 - dim))
    return level


def shared_out(key, own, number, rows, amount, top, reach, lean):
    sequence = jax.random.permutation(key, amount)
    crowded, usual = load_shares(amount, rows * top, reach, lean, True), load_shares(amount, rows * top, reach, lean, False)
    places = jnp.arange(amount)

    def named(tallies, offset_by):
        used = int((tallies > 0).sum())
        fixed = max(1, used // 4)
        shifted = fixed + (places - fixed + offset_by * (used - fixed)) % max(1, amount - fixed)
        return jnp.zeros((amount,), jnp.int32).at[sequence[jnp.where(places < fixed, places, shifted)]].set(jnp.asarray(tallies, jnp.int32))

    tallies = jnp.where(number % 4 == 0, named(crowded, number // 4), named(usual, number - number // 4 - 1))
    mixed = jax.random.permutation(jax.random.fold_in(own, 3), amount)
    donor, taker = mixed[0:amount // 2 * 2:2], mixed[1:amount // 2 * 2:2]
    margin = jnp.minimum(tallies[donor] - 1, reach - tallies[taker]) // 2
    margin = jnp.where((donor == sequence[0]) | (taker == sequence[0]) | (tallies[taker] == 0), 0, jnp.maximum(margin, 0))
    shifted = jax.random.randint(jax.random.fold_in(own, 4), (amount // 2,), 0, 1 << 20) % (margin + 1)
    tallies = tallies.at[donor].add(-shifted).at[taker].add(shifted)
    items = jnp.searchsorted(jnp.cumsum(tallies), jnp.arange(rows * top), side="right").astype(jnp.int32)
    table = items.reshape(top, rows).T
    table = table[jax.random.permutation(jax.random.fold_in(own, 1), rows)]
    offset_by = jax.random.randint(jax.random.fold_in(own, 2), (rows, 1), 0, top)
    return jnp.take_along_axis(table, (jnp.arange(top)[None, :] + offset_by) % top, axis=1)


def load_shares(number_of, total, reach, slope, full):
    loads = [(1 << 20) // math.isqrt(grade ** slope) + 1 for grade in range(1, number_of + 1)]
    largest = reach if full else min(reach, max(-(-total // number_of), total * loads[0] // sum(loads)))
    least = 1 if total - largest >= number_of - 1 else 0
    holding, surplus = [largest] + [least] * (number_of - 1), total - largest - least * (number_of - 1)
    while surplus > 0:
        free = [i for i in range(1, number_of) if holding[i] < largest] or [i for i in range(1, number_of) if holding[i] < reach]
        mass, remaining = sum([loads[i] for i in free]), surplus
        for i in free:
            addition = min(reach - holding[i], max(1, remaining * loads[i] // mass), surplus)
            holding[i] = holding[i] + addition
            surplus = surplus - addition
    return np.array(holding)


def centred(rng, dims, scale, limit, shards=(), held_as=jnp.bfloat16):
    result = jax.random.normal(rng, dims, jnp.float32) * scale
    if len(shards) > 0:
        result = levels(rng, dims, shards, -0.22, 0.18) * result
    return jnp.clip(result, min=-limit, max=limit).astype(held_as)


def setup_inputs(seed: int = 0) -> dict:
    seeds = jax.random.split(jax.random.key(seed), 13)
    tokens = centred(seeds[0], (TOKENS, D), 1.0, 6.0, ((0, 32), (1, 16)))
    norm_gain = jnp.clip(1.0 + 0.18 * jax.random.normal(seeds[1], (D,), jnp.float32), 0.1, 1.9)
    route_experts_keys = jax.random.split(jax.random.fold_in(seeds[2], 1), TOKENS // TOK_DEV)
    route_experts_turns = jax.random.permutation(jax.random.fold_in(seeds[2], 3), TOKENS // TOK_DEV)
    route_experts = jax.vmap(lambda own, number: shared_out(jax.random.fold_in(seeds[2], 2), own, number, TOK_DEV, EXPERTS, TOP, CAP, 2))(route_experts_keys, route_experts_turns).reshape((TOKENS, TOP))
    route_logits = centred(seeds[3], (TOKENS, TOP), 1.0, 4.0, ((0, 32),), jnp.float32)
    expert_gate = centred(seeds[4], (EXPERTS, D, FFE), D ** -0.5, 0.09375, ((0, 32), (2, 16)))
    expert_up = centred(seeds[5], (EXPERTS, D, FFE), D ** -0.5, 0.09375, ((0, 32), (2, 16)))
    expert_down = centred(seeds[6], (EXPERTS, FFE, D), FFE ** -0.5, 0.1875, ((0, 32), (1, 16)))
    dense_gate = centred(seeds[7], (D, DENSE_FF), D ** -0.5, 0.09375, ((1, 16),))
    dense_up = centred(seeds[8], (D, DENSE_FF), D ** -0.5, 0.09375, ((1, 16),))
    dense_down = centred(seeds[9], (DENSE_FF, D), DENSE_FF ** -0.5, 0.1875, ((0, 16),))
    mix_weight = centred(seeds[10], (D,), D ** -0.5, 0.09375, (), jnp.float32)
    out_gain = jnp.clip(1.0 + 0.18 * jax.random.normal(seeds[11], (D,), jnp.float32), 0.1, 1.9)
    return dict(tokens=tokens, norm_gain=norm_gain, route_experts=route_experts, route_logits=route_logits, expert_gate=expert_gate, expert_up=expert_up, expert_down=expert_down, dense_gate=dense_gate, dense_up=dense_up, dense_down=dense_down, mix_weight=mix_weight, out_gain=out_gain)


norm_eps = 1e-06

def reference(tokens, norm_gain, route_experts, route_logits, expert_gate, expert_up, expert_down, dense_gate, dense_up, dense_down, mix_weight, out_gain):
    values = tokens.astype(jnp.float32)
    normed = (values * lax.rsqrt(lax.optimization_barrier(jnp.mean(values * values, axis=1, keepdims=True)) + norm_eps) * norm_gain).astype(jnp.bfloat16)
    weights = jax.nn.softmax(route_logits, axis=-1)
    rows_cap = N_EP * CAP

    def per_expert(running, expert):
        route_hits = route_experts == expert
        routed = jnp.any(route_hits, axis=1)
        row_index = jnp.nonzero(routed, size=rows_cap, fill_value=0)[0].astype(jnp.int32)
        row_count = jnp.sum(routed.astype(jnp.int32))
        usable = (jnp.arange(rows_cap, dtype=jnp.int32) < row_count).astype(jnp.float32)
        picked = normed[row_index]
        gate_act = jnp.dot(picked, expert_gate[expert], preferred_element_type=jnp.float32)
        up_act = jnp.dot(picked, expert_up[expert], preferred_element_type=jnp.float32)
        hidden = (jax.nn.silu(gate_act) * up_act).astype(jnp.bfloat16)
        produced = jnp.dot(hidden, expert_down[expert], preferred_element_type=jnp.float32)
        factor = lax.optimization_barrier(jnp.sum(jnp.where(route_hits, weights, jnp.zeros_like(weights)), axis=1))[row_index] * usable
        return (running.at[row_index].add(factor[:, None] * produced), None)
    expert_mix, _ = lax.scan(per_expert, jnp.zeros((TOKENS, D), jnp.float32), jnp.arange(EXPERTS, dtype=jnp.int32))
    dense_hidden = (jax.nn.silu(jnp.dot(normed, dense_gate, preferred_element_type=jnp.float32)) * jnp.dot(normed, dense_up, preferred_element_type=jnp.float32)).astype(jnp.bfloat16)
    dense_out = jnp.dot(dense_hidden, dense_down, preferred_element_type=jnp.float32)
    mix_gate = jax.nn.sigmoid(jnp.dot(normed.astype(jnp.float32), mix_weight, precision=lax.Precision.HIGHEST))
    combined = expert_mix + mix_gate[:, None] * dense_out
    scaled = combined * lax.rsqrt(lax.optimization_barrier(jnp.mean(combined * combined, axis=1, keepdims=True)) + norm_eps) * out_gain
    return scaled.astype(jnp.bfloat16)
```

```python
import functools

import jax
import jax.numpy as jnp
from jax import lax
from jax.experimental import pallas as pl
from jax.experimental.pallas import tpu as pltpu
from jax.sharding import PartitionSpec as P

CAP = 2
CORES = 2
NX = 4
norm_eps = 1e-06
MESH = pl.DeviceIdType.MESH
F32 = jnp.float32
BF16 = jnp.bfloat16
NT = (((1,), (1,)), ((), ()))


def silu(v):
    return v / (1.0 + jnp.exp(-v))


def far_first(i, n):
    half = (i + 1) // 2
    return n // 2 - half if i % 2 == 1 else (n // 2 + half) % n


def far_first_vec(i, n):
    half = (i + 1) >> 1
    return jnp.where((i & 1) == 1, n // 2 - half, (n // 2 + half) & (n - 1))


def kernel(
    n_ep,
    n_tp,
    n_loc,
    tok_hbm,
    gain_hbm,
    route_hbm,
    logit_hbm,
    eg_hbm,
    eu_hbm,
    ed_hbm,
    dg_hbm,
    du_hbm,
    dd_hbm,
    mix_hbm,
    og_hbm,
    out_ref,
    tok,
    gain,
    route,
    logit,
    wgu,
    ed,
    wd,
    dd,
    mixw,
    og,
    normed,
    stacked,
    disp_send,
    own_recv,
    par_recv,
    rows_n,
    hid4,
    dense_send,
    dense_recv,
    pair_send,
    pair_recv,
    ret_send,
    ret_recv,
    scl_send,
    scl_recv,
    fin_send,
    fin_recv,
    sq_send,
    sq_recv,
    lsem,
    esem,
    ag_s,
    ag_r,
    di_s,
    di_r,
    pf_s,
    pf_r,
    de_s,
    de_r,
    pa_s,
    pa_r,
    re_s,
    re_r,
    sc_s,
    sc_r,
    fi_s,
    fi_r,
    sq_s,
    sq_r,
):
    me = lax.axis_index("ep")
    tp = lax.axis_index("tp")
    core = lax.rem(tp, CORES)
    row = lax.div(tp, CORES)
    n_row = n_tp // CORES
    partner = row * CORES + (1 - core)
    t_rows, part = tok.shape[1], tok.shape[2]
    width = part * n_tp
    nx = min(NX, n_ep)
    nz = n_ep // nx
    my_z = lax.div(me, nx)
    my_x = lax.rem(me, nx)
    slot = n_loc * CAP
    nq = n_row // 2
    blk = nq * slot
    slots = n_ep * blk
    wide = 2 * part
    keys = nq * t_rows
    hid = ed.shape[1] // nq
    n_chunk = 4 if n_ep >= 8 else 2
    per = n_ep // n_chunk
    crow = per * blk
    xrow = per * slot

    def turn(base, d, n):
        return lax.rem(base + d, n)

    def remote(src, dst, s, r, e, t):
        return pltpu.make_async_remote_copy(
            src_ref=src,
            dst_ref=dst,
            send_sem=s,
            recv_sem=r,
            device_id={"ep": e, "tp": t},
            device_id_type=MESH,
        )

    def offsets(b):
        return far_first(b // nx, nz), far_first(b % nx, nx)

    def ahead(b):
        dz, dx = offsets(b)
        return turn(my_z, dz, nz) * nx + turn(my_x, dx, nx)

    def behind(b):
        dz, dx = offsets(b)
        return turn(my_z, (nz - dz) % nz, nz) * nx + turn(my_x, (nx - dx) % nx, nx)

    def natural(q, h, g):
        return CORES * (2 * q + h) + g

    barrier = pltpu.get_barrier_semaphore()
    greeted = 0
    for d in range(1, n_ep):
        pl.semaphore_signal(
            barrier, inc=1, device_id={"ep": turn(me, d, n_ep), "tp": tp}, device_id_type=MESH
        )
        greeted += 1
    for d in range(1, n_tp):
        pl.semaphore_signal(
            barrier, inc=1, device_id={"ep": me, "tp": turn(tp, d, n_tp)}, device_id_type=MESH
        )
        greeted += 1

    half_w = wgu.shape[0] // 2
    ffd = wd.shape[0] // 2
    loads = []
    pairs = [
        (tok_hbm, tok.at[tp]),
        (route_hbm, route),
        (logit_hbm, logit),
        (gain_hbm, gain),
        (mix_hbm, mixw),
        (og_hbm, og),
        (dg_hbm, wd.at[0:ffd]),
        (du_hbm, wd.at[ffd : 2 * ffd]),
        (dd_hbm, dd),
        (eg_hbm, wgu.at[0:half_w]),
        (eu_hbm, wgu.at[half_w : 2 * half_w]),
    ]
    for i, (src, dst) in enumerate(pairs):
        c = pltpu.make_async_copy(src, dst, lsem.at[i])
        c.start()
        loads.append(c)
    ed_loads = []
    for g in range(CORES):
        for q in range(nq):
            for h in range(2):
                t = natural(q, h, g)
                c = pltpu.make_async_copy(
                    ed_hbm.at[:, t * part : (t + 1) * part],
                    ed.at[g, q * hid : (q + 1) * hid, h * part : (h + 1) * part],
                    esem.at[t],
                )
                c.start()
                ed_loads.append(c)

    gathers = []
    for d in range(1, n_tp):
        gathers.append(
            remote(tok.at[tp], tok.at[tp], ag_s.at[d], ag_r.at[d], me, turn(tp, d, n_tp))
        )

    loads[1].wait()
    loads[2].wait()
    spread = (
        lax.broadcasted_iota(jnp.int32, (t_rows, keys), 0)
        == (lax.broadcasted_iota(jnp.int32, (t_rows, keys), 1) & (t_rows - 1))
    ).astype(F32)

    def tiled(v):
        return jnp.dot(v, spread, preferred_element_type=F32, precision=lax.Precision.HIGHEST)

    l0 = logit[0:1, :]
    l1 = logit[1:2, :]
    top = jnp.maximum(l0, l1)
    e0 = jnp.exp(l0 - top)
    e1 = jnp.exp(l1 - top)
    w0 = tiled(e0 / (e0 + e1))
    w1 = tiled(e1 / (e0 + e1))
    r0 = tiled(route[0:1, :].astype(F32))
    r1 = tiled(route[1:2, :].astype(F32))
    ri = lax.broadcasted_iota(jnp.int32, (keys, keys), 0)
    ci = lax.broadcasted_iota(jnp.int32, (keys, keys), 1)
    tri = ((ri < ci) & ((ri // t_rows) == (ci // t_rows))).astype(F32)
    r = lax.broadcasted_iota(jnp.int32, (slots, keys), 0)
    k = lax.broadcasted_iota(jnp.int32, (slots, keys), 1)
    b = r // blk
    s = r % slot
    dz = far_first_vec(b // nx, nz)
    dx = far_first_vec(b % nx, nx)
    dest = ((my_z + dz) & (nz - 1)) * nx + ((my_x + dx) & (nx - 1))
    slot_e = (dest * n_loc + s // CAP).astype(F32)
    same = ((r // slot) % nq) == (k // t_rows)
    hit0 = (slot_e == r0).astype(F32)
    hit1 = (slot_e == r1).astype(F32)
    hits = hit0 + hit1
    before = jnp.dot(hits, tri, preferred_element_type=F32)
    place = jnp.where(same & (before == (s % CAP).astype(F32)), hits, 0.0)
    combine = (place * (hit0 * w0 + hit1 * w1)).T
    place = place.astype(BF16)

    pr = lax.broadcasted_iota(jnp.int32, (crow, crow), 0)
    pc = lax.broadcasted_iota(jnp.int32, (crow, crow), 1)
    perm = (
        ((pr // xrow) == ((pc // slot) % nq))
        & (((pr // slot) % per) == (pc // blk))
        & ((pr % slot) == (pc % slot))
    ).astype(BF16)
    xr = lax.broadcasted_iota(jnp.int32, (crow, xrow), 0)
    xc = lax.broadcasted_iota(jnp.int32, (crow, xrow), 1)
    expand = (((xr // blk) == (xc // slot)) & ((xr % slot) == (xc % slot))).astype(BF16)
    sr = lax.broadcasted_iota(jnp.int32, (crow, 128), 0)
    scol = lax.broadcasted_iota(jnp.int32, (crow, 128), 1)
    in_lane = (sr % blk) == scol
    gr = lax.broadcasted_iota(jnp.int32, (per, crow), 0)
    gc = lax.broadcasted_iota(jnp.int32, (per, crow), 1)
    in_block = gr == (gc // blk)
    br = lax.broadcasted_iota(jnp.int32, (128, crow), 0)
    bc = lax.broadcasted_iota(jnp.int32, (128, crow), 1)
    unlane = (br == (bc % blk)).astype(BF16)

    loads[0].wait()
    pl.semaphore_wait(barrier, greeted)
    for c in gathers:
        c.start()
    loads[3].wait()
    loads[4].wait()
    loads[5].wait()
    for c in gathers:
        c.wait_recv()
    squares = jnp.zeros((t_rows, part), F32)
    for t in range(n_tp):
        x = tok[t].astype(F32)
        squares += x * x
    inv = lax.rsqrt(jnp.sum(squares, axis=1, keepdims=True) / width + norm_eps)
    for t in range(n_tp):
        cols = slice(t * part, (t + 1) * part)
        normed[:, cols] = (tok[t].astype(F32) * inv * gain[:, cols]).astype(BF16)
    for q in range(nq):
        for h in range(2):
            cols = pl.ds(pl.multiple_of(natural(q, h, core) * part, part), part)
            stacked[q * t_rows : (q + 1) * t_rows, h * part : (h + 1) * part] = normed[
                :, cols
            ].astype(F32)
    source = stacked[...].astype(BF16)
    for c in range(n_chunk):
        rows = slice(c * crow, (c + 1) * crow)
        piece = jnp.dot(place[rows, :], source, preferred_element_type=F32).astype(BF16)
        disp_send[rows, :] = piece
        for i in range(per):
            j = c * per + i
            if j < n_ep - 1:
                at = pl.ds(j * blk, blk)
                remote(
                    disp_send.at[at], own_recv.at[at], di_s, di_r.at[c], ahead(j), tp
                ).start()
    tail = slice((n_ep - 1) * blk, n_ep * blk)
    own_recv[tail, :] = disp_send[tail, :]

    mix = jnp.sum(normed[...].astype(F32) * mixw[...], axis=1, keepdims=True)
    mix_gate = 1.0 / (1.0 + jnp.exp(-mix))
    for i in (6, 7, 8):
        loads[i].wait()
    both = lax.dot_general(normed[...], wd[...], NT, preferred_element_type=F32)
    dh = (silu(both[:, 0:ffd]) * both[:, ffd : 2 * ffd]).astype(BF16)
    for t in range(n_tp):
        dense_send[t] = jnp.dot(
            dh, dd[:, t * part : (t + 1) * part], preferred_element_type=F32
        )
    dense = []
    for d in range(1, n_tp):
        t = turn(tp, d, n_tp)
        c = remote(dense_send.at[t], dense_recv.at[tp], de_s.at[d], de_r.at[d], me, t)
        c.start()
        dense.append(c)
    dense_recv[tp] = dense_send[tp]
    for i in (9, 10):
        loads[i].wait()
    for c in ed_loads:
        c.wait()

    def unpack(src, c, g):
        rows = slice(c * crow, (c + 1) * crow)
        moved = jnp.dot(perm, src[rows, :], preferred_element_type=F32).astype(BF16)
        for q in range(nq):
            for h in range(2):
                cols = pl.ds(pl.multiple_of(natural(q, h, g) * part, part), part)
                rows_n[c * xrow : (c + 1) * xrow, cols] = moved[
                    q * xrow : (q + 1) * xrow, h * part : (h + 1) * part
                ]

    forwards = []
    for c in range(n_chunk):
        n = per - (c == n_chunk - 1)
        at = pl.ds(c * crow, n * blk)
        remote(disp_send.at[at], own_recv.at[at], di_s, di_r.at[c], me, tp).wait_recv()
        at = pl.ds(c * crow, crow)
        f = remote(own_recv.at[at], par_recv.at[at], pf_s.at[c], pf_r.at[c], me, partner)
        f.start()
        forwards.append(f)
        unpack(own_recv, c, core)
    for c in range(n_chunk):
        forwards[c].wait_recv()
        unpack(par_recv, c, 1 - core)
    act = lax.dot_general(rows_n[...], wgu[...], NT, preferred_element_type=F32)
    ar = lax.broadcasted_iota(jnp.int32, (n_ep * slot, hid), 0)
    ac = lax.broadcasted_iota(jnp.int32, (n_ep * slot, hid), 1)
    mine = ((ar % slot) // CAP) == (ac // (hid // n_loc))
    hidden = jnp.where(mine, silu(act[:, 0:hid]) * act[:, hid : 2 * hid], 0.0).astype(BF16)
    hr = lax.broadcasted_iota(jnp.int32, (crow, hid), 0)
    for c in range(n_chunk):
        wider = jnp.dot(
            expand, hidden[c * xrow : (c + 1) * xrow, :], preferred_element_type=F32
        )
        for q in range(nq):
            hid4[c * crow : (c + 1) * crow, q * hid : (q + 1) * hid] = jnp.where(
                ((hr // slot) % nq) == q, wider, 0.0
            ).astype(BF16)

    duo = []
    for c in range(n_chunk):
        rows = slice(c * crow, (c + 1) * crow)
        pair_send[rows, :] = jnp.dot(hid4[rows, :], ed[1 - core], preferred_element_type=F32)
        at = pl.ds(c * crow, crow)
        f = remote(pair_send.at[at], pair_recv.at[at], pa_s.at[c], pa_r.at[c], me, partner)
        f.start()
        duo.append(f)
    for c in range(n_chunk):
        rows = slice(c * crow, (c + 1) * crow)
        v = jnp.dot(hid4[rows, :], ed[core], preferred_element_type=F32)
        duo[c].wait_recv()
        v = v + pair_recv[rows, :]
        peak = jnp.max(jnp.abs(v), axis=1, keepdims=True)
        step = (jnp.maximum(peak, 1e-30) * (1.0 / 32600.0)).astype(BF16).astype(F32)
        ret_send[rows, :] = (
            jnp.floor(v * (1.0 / step) + 0.5).astype(jnp.int32).astype(jnp.int16)
        )
        lanes = jnp.where(in_lane, step, 0.0).astype(BF16)
        steps = jnp.dot(in_block.astype(BF16), lanes, preferred_element_type=F32)
        for i in range(per):
            j = c * per + i
            scl_send[j] = steps[i : i + 1, :]
            if j < n_ep - 1:
                at = pl.ds(j * blk, blk)
                remote(
                    ret_send.at[at], ret_recv.at[at], re_s, re_r.at[c], behind(j), tp
                ).start()
                remote(
                    scl_send.at[j], scl_recv.at[j], sc_s, sc_r.at[c], behind(j), tp
                ).start()
    ret_recv[tail, :] = ret_send[tail, :]
    scl_recv[n_ep - 1] = scl_send[n_ep - 1]

    for c in dense:
        c.wait_recv()
    total = dense_recv[0]
    for t in range(1, n_tp):
        total += dense_recv[t]
    total = mix_gate * total

    mixed = jnp.zeros((keys, wide), F32)
    for c in range(n_chunk):
        n = per - (c == n_chunk - 1)
        at = pl.ds(c * crow, n * blk)
        remote(ret_send.at[at], ret_recv.at[at], re_s, re_r.at[c], me, tp).wait_recv()
        at = pl.ds(c * per, n)
        remote(scl_send.at[at], scl_recv.at[at], sc_s, sc_r.at[c], me, tp).wait_recv()
        rows = slice(c * crow, (c + 1) * crow)
        steps = jnp.concatenate([scl_recv[c * per + i] for i in range(per)], axis=0)
        lanes = jnp.dot(steps.astype(BF16), unlane, preferred_element_type=F32)
        step = jnp.sum(jnp.where(in_block, lanes, 0.0), axis=0, keepdims=True)
        back = ret_recv[rows, :].astype(jnp.int32).astype(F32)
        mixed += jnp.dot(
            combine[:, rows] * step,
            back,
            preferred_element_type=F32,
            precision=lax.Precision.HIGHEST,
        )
    for q in range(nq):
        for h in range(2):
            fin_send[2 * q + h] = mixed[
                q * t_rows : (q + 1) * t_rows, h * part : (h + 1) * part
            ]
    finals = []
    for d in range(1, n_row):
        y = turn(row, d, n_row)
        c = remote(
            fin_send.at[y], fin_recv.at[row], fi_s.at[d], fi_r.at[d], me, y * CORES + core
        )
        c.start()
        finals.append(c)
    fin_recv[row] = fin_send[row]
    for c in finals:
        c.wait_recv()
    for y in range(n_row):
        total += fin_recv[y]
    sq_send[...] = jnp.broadcast_to(
        jnp.sum(total * total, axis=1, keepdims=True), sq_send.shape
    )
    swaps = []
    for d in range(1, n_tp):
        c = remote(sq_send, sq_recv.at[tp], sq_s.at[d], sq_r.at[d], me, turn(tp, d, n_tp))
        c.start()
        swaps.append(c)
    sq_recv[tp] = sq_send[...]
    for c in swaps:
        c.wait_recv()
    all_sq = sq_recv[0]
    for t in range(1, n_tp):
        all_sq += sq_recv[t]
    scale = lax.rsqrt(all_sq[:, 0:1] / width + norm_eps)
    out_ref[...] = (total * scale * og[...]).astype(out_ref.dtype)
    for c in gathers + forwards + dense + duo + finals + swaps:
        c.wait_send()
    at = pl.ds(0, (n_ep - 1) * blk)
    remote(disp_send.at[at], own_recv.at[at], di_s, di_r.at[0], me, tp).wait_send()
    remote(ret_send.at[at], ret_recv.at[at], re_s, re_r.at[0], me, tp).wait_send()
    at = pl.ds(0, n_ep - 1)
    remote(scl_send.at[at], scl_recv.at[at], sc_s, sc_r.at[0], me, tp).wait_send()


def shards(n_ep, n_tp, *args):
    (tok, gain, route, logit, eg, eu, ed, dg, du, dd, mixw, og) = args
    t_rows, part = tok.shape
    width = part * n_tp
    n_loc, _, ff = eg.shape
    ffd = dg.shape[1]
    hid = n_loc * ff
    n_row = n_tp // CORES
    nq = n_row // 2
    slot = n_loc * CAP
    blk = nq * slot
    slots = n_ep * blk
    wide = 2 * part
    n_chunk = 4 if n_ep >= 8 else 2
    dma = pltpu.SemaphoreType.DMA
    V = pltpu.VMEM
    scratch = [
        V((n_tp, t_rows, part), BF16),
        V((1, width), F32),
        V(route.shape[::-1], jnp.int32),
        V(logit.shape[::-1], F32),
        V((2 * hid, width), BF16),
        V((CORES, nq * hid, wide), BF16),
        V((2 * ffd, width), BF16),
        V(dd.shape, BF16),
        V((1, width), F32),
        V((1, part), F32),
        V((t_rows, width), BF16),
        V((nq * t_rows, wide), F32),
        V((slots, wide), BF16),
        V((slots, wide), BF16),
        V((slots, wide), BF16),
        V((n_ep * slot, width), BF16),
        V((slots, nq * hid), BF16),
        V((n_tp, t_rows, part), F32),
        V((n_tp, t_rows, part), F32),
        V((slots, wide), F32),
        V((slots, wide), F32),
        V((slots, wide), jnp.int16),
        V((slots, wide), jnp.int16),
        V((n_ep, 1, 128), F32),
        V((n_ep, 1, 128), F32),
        V((n_row, t_rows, part), F32),
        V((n_row, t_rows, part), F32),
        V((t_rows, 128), F32),
        V((n_tp, t_rows, 128), F32),
        dma((11,)),
        dma((n_tp,)),
        dma((n_tp,)),
        dma((n_tp,)),
        dma,
        dma((n_chunk,)),
        dma((n_chunk,)),
        dma((n_chunk,)),
        dma((n_tp,)),
        dma((n_tp,)),
        dma((n_chunk,)),
        dma((n_chunk,)),
        dma,
        dma((n_chunk,)),
        dma,
        dma((n_chunk,)),
        dma((n_row,)),
        dma((n_row,)),
        dma((n_tp,)),
        dma((n_tp,)),
    ]
    return pl.pallas_call(
        functools.partial(kernel, n_ep, n_tp, n_loc),
        out_shape=jax.ShapeDtypeStruct((t_rows, part), BF16),
        in_specs=[pl.BlockSpec(memory_space=pltpu.HBM)] * 12,
        out_specs=pl.BlockSpec(memory_space=pltpu.VMEM),
        scratch_shapes=scratch,
        compiler_params=pltpu.CompilerParams(
            collective_id=0, has_side_effects=True, vmem_limit_bytes=60 * 1024 * 1024
        ),
        name="moe_layer",
    )(
        tok,
        gain.reshape(1, width),
        route.T,
        logit.T,
        eg.swapaxes(1, 2).reshape(hid, width),
        eu.swapaxes(1, 2).reshape(hid, width),
        ed.reshape(hid, width),
        dg.T,
        du.T,
        dd,
        mixw.reshape(1, width),
        og.reshape(1, part),
    )


def solution(mesh):
    placed = (
        P("ep", "tp"),
        P(),
        P("ep", None),
        P("ep", None),
        P("ep", None, "tp"),
        P("ep", None, "tp"),
        P("ep", "tp", None),
        P(None, "tp"),
        P(None, "tp"),
        P("tp", None),
        P(),
        P("tp"),
    )
    return jax.shard_map(
        functools.partial(shards, mesh.shape["ep"], mesh.shape["tp"]),
        mesh=mesh,
        in_specs=placed,
        out_specs=P("ep", "tp"),
        check_vma=False,
    )
```

```python
import functools

import jax
import jax.numpy as jnp
from jax import lax
from jax.experimental import pallas as pl
from jax.experimental.pallas import tpu as pltpu
from jax.sharding import PartitionSpec as P

CAP = 2
CORES = 2
NX = 4
CHUNKS = 4
norm_eps = 1e-06
MESH = pl.DeviceIdType.MESH
F32 = jnp.float32
BF16 = jnp.bfloat16
NT = (((1,), (1,)), ((), ()))


def silu(v):
    return v / (1.0 + jnp.exp(-v))


def chunks_of(n_ep):
    return CHUNKS if n_ep >= 2 * CHUNKS else 2


def far_first(i, n):
    half = (i + 1) // 2
    return n // 2 - half if i % 2 == 1 else (n // 2 + half) % n


def far_first_vec(i, n):
    half = (i + 1) >> 1
    return jnp.where((i & 1) == 1, n // 2 - half, (n // 2 + half) & (n - 1))


def kernel(
    n_ep,
    n_tp,
    n_loc,
    tok_hbm,
    gain_hbm,
    route_hbm,
    logit_hbm,
    eg_hbm,
    eu_hbm,
    ed_hbm,
    dg_hbm,
    du_hbm,
    dd_hbm,
    mix_hbm,
    og_hbm,
    out_ref,
    tok,
    gain,
    route,
    logit,
    wgu,
    ednat,
    ed,
    wd,
    dd,
    mixw,
    og,
    normed,
    disp_send,
    grid,
    rows_n,
    hid4,
    dense_send,
    dense_recv,
    pair_send,
    pair_recv,
    ret_send,
    ret_recv,
    scl_send,
    scl_recv,
    fin_send,
    fin_recv,
    sq_send,
    sq_recv,
    lsem,
    ag_s,
    ag_r,
    di_s,
    di_r,
    ya_s,
    ya_r,
    pf_s,
    pf_r,
    de_s,
    de_r,
    pa_s,
    pa_r,
    re_s,
    re_r,
    sc_s,
    sc_r,
    fi_s,
    fi_r,
    sq_s,
    sq_r,
):
    me = lax.axis_index("ep")
    tp = lax.axis_index("tp")
    core = lax.rem(tp, CORES)
    row = lax.div(tp, CORES)
    n_row = n_tp // CORES
    partner = row * CORES + (1 - core)
    t_rows, part = tok.shape[1], tok.shape[2]
    width = part * n_tp
    half = part // 2
    nx = min(NX, n_ep)
    nz = n_ep // nx
    my_z = lax.div(me, nx)
    my_x = lax.rem(me, nx)
    slot = n_loc * CAP
    blk = 2 * slot
    slots = n_ep * blk
    keys = 2 * t_rows
    hid = ednat.shape[0]
    n_chunk = chunks_of(n_ep)
    order = [n_chunk - 1] + list(range(n_chunk - 1))
    per = n_ep // n_chunk
    crow = per * blk
    xrow = per * slot
    nq = n_row // 2
    big = nq * slot
    brow = per * big
    wide = 2 * part
    far_rows = sorted(range(1, n_row), key=lambda d: -min(d, n_row - d))
    far_tp = sorted(range(1, n_tp), key=lambda d: -min(d, n_tp - d))

    def turn(base, d, n):
        return lax.rem(base + d, n)

    def remote(src, dst, s, r, e, t):
        return pltpu.make_async_remote_copy(
            src_ref=src,
            dst_ref=dst,
            send_sem=s,
            recv_sem=r,
            device_id={"ep": e, "tp": t},
            device_id_type=MESH,
        )

    def offsets(b):
        return far_first(b // nx, nz), far_first(b % nx, nx)

    def ahead(b):
        dz, dx = offsets(b)
        return turn(my_z, dz, nz) * nx + turn(my_x, dx, nx)

    def behind(b):
        dz, dx = offsets(b)
        return turn(my_z, (nz - dz) % nz, nz) * nx + turn(my_x, (nx - dx) % nx, nx)

    def chunk(c):
        return pl.ds(c * per, per)

    barrier = pltpu.get_barrier_semaphore()
    greeted = 0
    for j in range(n_ep - 1):
        pl.semaphore_signal(
            barrier, inc=1, device_id={"ep": ahead(j), "tp": tp}, device_id_type=MESH
        )
        greeted += 1
    for d in far_tp:
        pl.semaphore_signal(
            barrier, inc=1, device_id={"ep": me, "tp": turn(tp, d, n_tp)}, device_id_type=MESH
        )
        greeted += 1

    half_w = wgu.shape[0] // 2
    ffd = wd.shape[0] // 2
    loads = []
    pairs = [
        (tok_hbm, tok.at[tp]),
        (route_hbm, route),
        (logit_hbm, logit),
        (gain_hbm, gain),
        (mix_hbm, mixw),
        (og_hbm, og),
        (dg_hbm, wd.at[0:ffd]),
        (du_hbm, wd.at[ffd : 2 * ffd]),
        (dd_hbm, dd),
        (ed_hbm, ednat),
        (eg_hbm, wgu.at[0:half_w]),
        (eu_hbm, wgu.at[half_w : 2 * half_w]),
    ]
    for i, (src, dst) in enumerate(pairs):
        c = pltpu.make_async_copy(src, dst, lsem.at[i])
        c.start()
        loads.append(c)

    loads[1].wait()
    spread = (
        lax.broadcasted_iota(jnp.int32, (t_rows, keys), 0)
        == (lax.broadcasted_iota(jnp.int32, (t_rows, keys), 1) % t_rows)
    ).astype(F32)
    both = jnp.dot(route[...].astype(F32), spread, preferred_element_type=F32)
    ri = lax.broadcasted_iota(jnp.int32, (keys, keys), 0)
    ci = lax.broadcasted_iota(jnp.int32, (keys, keys), 1)
    tri = ((ri < ci) & ((ri // t_rows) == (ci // t_rows))).astype(F32)
    r = lax.broadcasted_iota(jnp.int32, (slots, keys), 0)
    k = lax.broadcasted_iota(jnp.int32, (slots, keys), 1)
    b = r // blk
    s = r % slot
    dz = far_first_vec(b // nx, nz)
    dx = far_first_vec(b % nx, nx)
    dest = ((my_z + dz) & (nz - 1)) * nx + ((my_x + dx) & (nx - 1))
    slot_e = (dest * n_loc + s // CAP).astype(F32)
    same = ((r // slot) % 2) == (k // t_rows)
    hit0 = (slot_e == both[0:1, :]).astype(F32)
    hit1 = (slot_e == both[1:2, :]).astype(F32)
    hits = hit0 + hit1
    before = jnp.dot(hits, tri, preferred_element_type=F32)
    place = jnp.where(same & (before == (s % CAP).astype(F32)), hits, 0.0)
    loads[0].wait()
    x = tok[tp].astype(F32)
    source = jnp.concatenate([x[:, 0:half], x[:, half:part]], axis=0).astype(BF16)
    placed = jnp.dot(place.astype(BF16), source, preferred_element_type=F32)
    placed = placed.reshape(n_ep, blk, half).astype(BF16)
    disp_send[...] = placed
    pl.semaphore_wait(barrier, greeted)
    for j in range(n_ep - 1):
        remote(
            disp_send.at[j], grid.at[core, row, j], di_s, di_r.at[j // per], ahead(j), tp
        ).start()
    for d in far_tp:
        remote(tok.at[tp], tok.at[tp], ag_s, ag_r, me, turn(tp, d, n_tp)).start()
    grid[core, row, n_ep - 1] = placed[n_ep - 1]

    loads[2].wait()
    l0 = logit[0:1, :]
    l1 = logit[1:2, :]
    top = jnp.maximum(l0, l1)
    e0 = jnp.exp(l0 - top)
    e1 = jnp.exp(l1 - top)
    shares = jnp.concatenate([e0 / (e0 + e1), e1 / (e0 + e1)], axis=0)
    names = jnp.concatenate([route[...].astype(F32), shares], axis=0)
    bkeys = nq * t_rows
    bspread = (
        lax.broadcasted_iota(jnp.int32, (t_rows, bkeys), 0)
        == (lax.broadcasted_iota(jnp.int32, (t_rows, bkeys), 1) % t_rows)
    ).astype(F32)
    names = jnp.dot(
        names, bspread, preferred_element_type=F32, precision=lax.Precision.HIGHEST
    )
    ri = lax.broadcasted_iota(jnp.int32, (bkeys, bkeys), 0)
    ci = lax.broadcasted_iota(jnp.int32, (bkeys, bkeys), 1)
    tri = ((ri < ci) & ((ri // t_rows) == (ci // t_rows))).astype(F32)
    r = lax.broadcasted_iota(jnp.int32, (n_ep * big, bkeys), 0)
    k = lax.broadcasted_iota(jnp.int32, (n_ep * big, bkeys), 1)
    b = r // big
    s = r % slot
    dz = far_first_vec(b // nx, nz)
    dx = far_first_vec(b % nx, nx)
    dest = ((my_z + dz) & (nz - 1)) * nx + ((my_x + dx) & (nx - 1))
    slot_e = (dest * n_loc + s // CAP).astype(F32)
    same = ((r // slot) % nq) == (k // t_rows)
    hit0 = (slot_e == names[0:1, :]).astype(F32)
    hit1 = (slot_e == names[1:2, :]).astype(F32)
    before = jnp.dot(hit0 + hit1, tri, preferred_element_type=F32)
    taken = same & (before == (s % CAP).astype(F32))
    combine = jnp.where(taken, hit0 * names[2:3, :] + hit1 * names[3:4, :], 0.0).T
    pr = lax.broadcasted_iota(jnp.int32, (crow, crow), 0)
    pc = lax.broadcasted_iota(jnp.int32, (crow, crow), 1)
    perm = (
        ((pr // xrow) == ((pc // slot) % 2))
        & (((pr // slot) % per) == (pc // blk))
        & ((pr % slot) == (pc % slot))
    ).astype(BF16)
    xr = lax.broadcasted_iota(jnp.int32, (brow, xrow), 0)
    xc = lax.broadcasted_iota(jnp.int32, (brow, xrow), 1)
    expand = (((xr // big) == (xc // slot)) & ((xr % slot) == (xc % slot))).astype(BF16)
    sr = lax.broadcasted_iota(jnp.int32, (brow, 128), 0)
    sc = lax.broadcasted_iota(jnp.int32, (brow, 128), 1)
    in_lane = (sr % big) == sc
    gr = lax.broadcasted_iota(jnp.int32, (per, brow), 0)
    gc = lax.broadcasted_iota(jnp.int32, (per, brow), 1)
    in_block = gr == (gc // big)
    br = lax.broadcasted_iota(jnp.int32, (128, brow), 0)
    bc = lax.broadcasted_iota(jnp.int32, (128, brow), 1)
    unlane = (br == (bc % big)).astype(BF16)
    loads[9].wait()
    for g in range(CORES):
        for q in range(nq):
            for h in range(2):
                at = (CORES * (2 * q + h) + g) * part
                ed[g, q * hid : (q + 1) * hid, h * part : (h + 1) * part] = ednat[
                    :, at : at + part
                ]

    for c in order:
        at = pl.ds(c * per, per - (c == n_chunk - 1))
        remote(
            disp_send.at[at], grid.at[core, row, at], di_s, di_r.at[c], me, tp
        ).wait_recv()
        for d in far_rows:
            spot = grid.at[core, row, chunk(c)]
            remote(spot, spot, ya_s, ya_r.at[c], me, turn(row, d, n_row) * CORES + core).start()

    for i in (3, 4, 5):
        loads[i].wait()
    at = pl.ds(0, n_tp - 1)
    remote(tok.at[at], tok.at[at], ag_s, ag_r, me, tp).wait_recv()
    squares = jnp.zeros((t_rows, part), F32)
    for t in range(n_tp):
        x = tok[t].astype(F32)
        squares += x * x
    inv = lax.rsqrt(jnp.sum(squares, axis=1, keepdims=True) / width + norm_eps)
    mix = jnp.zeros((t_rows, part), F32)
    for t in range(n_tp):
        cols = slice(t * part, (t + 1) * part)
        nt = (tok[t].astype(F32) * inv * gain[:, cols]).astype(BF16)
        normed[:, cols] = nt
        mix += nt.astype(F32) * mixw[:, cols]
    mix_gate = 1.0 / (1.0 + jnp.exp(-jnp.sum(mix, axis=1, keepdims=True)))
    for i in (6, 7, 8):
        loads[i].wait()
    both = lax.dot_general(normed[...], wd[...], NT, preferred_element_type=F32)
    dh = (silu(both[:, 0:ffd]) * both[:, ffd : 2 * ffd]).astype(BF16)
    for t in range(n_tp):
        dense_send[t] = jnp.dot(
            dh, dd[:, t * part : (t + 1) * part], preferred_element_type=F32
        )
    for d in far_tp:
        t = turn(tp, d, n_tp)
        remote(dense_send.at[t], dense_recv.at[d - 1], de_s, de_r, me, t).start()
    for i in (10, 11):
        loads[i].wait()

    def unpack(c, g):
        slabs = [
            grid[g, y, c * per : (c + 1) * per].astype(F32).reshape(crow, half)
            for y in range(n_row)
        ]
        moved = jnp.dot(
            perm, jnp.concatenate(slabs, axis=1).astype(BF16), preferred_element_type=F32
        )
        total = jnp.zeros((xrow, half), F32)
        for y in range(n_row):
            for h in range(2):
                v = moved[h * xrow : (h + 1) * xrow, y * half : (y + 1) * half]
                at = pl.multiple_of((CORES * y + g) * part + h * half, half)
                rows_n[c * xrow : (c + 1) * xrow, pl.ds(at, half)] = v.astype(BF16)
                total += v * v
        return jnp.sum(total, axis=1, keepdims=True)

    ar = lax.broadcasted_iota(jnp.int32, (xrow, hid), 0)
    ac = lax.broadcasted_iota(jnp.int32, (xrow, hid), 1)
    mine = ((ar % slot) // CAP) == (ac // (hid // n_loc))
    hr = lax.broadcasted_iota(jnp.int32, (brow, hid), 0)
    seen = {}

    def gather(c):
        at = pl.ds(0, n_row - 1)
        spot = grid.at[core, at, chunk(c)]
        remote(spot, spot, ya_s, ya_r.at[c], me, tp).wait_recv()
        spot = grid.at[core, :, chunk(c)]
        remote(spot, spot, pf_s, pf_r.at[c], me, partner).start()
        seen[c] = unpack(c, core)

    def apply(c):
        spot = grid.at[1 - core, :, chunk(c)]
        remote(spot, spot, pf_s, pf_r.at[c], me, tp).wait_recv()
        inv = lax.rsqrt((seen[c] + unpack(c, 1 - core)) / width + norm_eps)
        rows = slice(c * xrow, (c + 1) * xrow)
        for t in range(n_tp):
            cols = slice(t * part, (t + 1) * part)
            rows_n[rows, cols] = (rows_n[rows, cols].astype(F32) * inv * gain[:, cols]).astype(
                BF16
            )
        act = lax.dot_general(rows_n[rows, :], wgu[...], NT, preferred_element_type=F32)
        hidden = jnp.where(mine, silu(act[:, 0:hid]) * act[:, hid : 2 * hid], 0.0)
        wider = jnp.dot(expand, hidden.astype(BF16), preferred_element_type=F32)
        rows = slice(c * brow, (c + 1) * brow)
        for q in range(nq):
            hid4[rows, q * hid : (q + 1) * hid] = jnp.where(
                ((hr // slot) % nq) == q, wider, 0.0
            ).astype(BF16)
        pair_send[rows, :] = jnp.dot(hid4[rows, :], ed[1 - core], preferred_element_type=F32)
        at = pl.ds(c * brow, brow)
        remote(pair_send.at[at], pair_recv.at[at], pa_s, pa_r.at[c], me, partner).start()

    def reply(c):
        rows = slice(c * brow, (c + 1) * brow)
        v = jnp.dot(hid4[rows, :], ed[core], preferred_element_type=F32)
        at = pl.ds(c * brow, brow)
        remote(pair_send.at[at], pair_recv.at[at], pa_s, pa_r.at[c], me, tp).wait_recv()
        v = v + pair_recv[rows, :]
        peak = jnp.max(jnp.abs(v), axis=1, keepdims=True)
        step = (jnp.maximum(peak, 1e-30) * (1.0 / 32600.0)).astype(BF16).astype(F32)
        ret_send[rows, :] = (
            jnp.floor(v * (1.0 / step) + 0.5).astype(jnp.int32).astype(jnp.int16)
        )
        lanes = jnp.where(in_lane, step, 0.0).astype(BF16)
        steps = jnp.dot(in_block.astype(BF16), lanes, preferred_element_type=F32)
        for i in range(per):
            j = c * per + i
            scl_send[j] = steps[i : i + 1, :]
            if j < n_ep - 1:
                at = pl.ds(j * big, big)
                remote(
                    ret_send.at[at], ret_recv.at[at], re_s, re_r.at[c], behind(j), tp
                ).start()
                remote(
                    scl_send.at[j], scl_recv.at[j], sc_s, sc_r.at[c], behind(j), tp
                ).start()
        if c == n_chunk - 1:
            tail = slice((n_ep - 1) * big, n_ep * big)
            ret_recv[tail, :] = ret_send[tail, :]
            scl_recv[n_ep - 1] = scl_send[n_ep - 1]

    steps = [gather, apply, reply]
    for tick in range(n_chunk + len(steps) - 1):
        for age, step in enumerate(steps):
            if 0 <= tick - age < n_chunk:
                step(order[tick - age])
    at = pl.ds(0, n_tp - 1)
    remote(dense_recv.at[at], dense_recv.at[at], de_s, de_r, me, tp).wait_recv()
    total = dense_send[tp]
    for d in range(1, n_tp):
        total += dense_recv[d - 1]
    total = mix_gate * total
    mixed = jnp.zeros((bkeys, wide), F32)
    for c in order:
        n = per - (c == n_chunk - 1)
        at = pl.ds(c * brow, n * big)
        remote(ret_send.at[at], ret_recv.at[at], re_s, re_r.at[c], me, tp).wait_recv()
        at = pl.ds(c * per, n)
        remote(scl_send.at[at], scl_recv.at[at], sc_s, sc_r.at[c], me, tp).wait_recv()
        rows = slice(c * brow, (c + 1) * brow)
        steps = jnp.concatenate([scl_recv[c * per + i] for i in range(per)], axis=0)
        lanes = jnp.dot(steps.astype(BF16), unlane, preferred_element_type=F32)
        step = jnp.sum(jnp.where(in_block, lanes, 0.0), axis=0, keepdims=True)
        back = ret_recv[rows, :].astype(jnp.int32).astype(F32)
        mixed += jnp.dot(
            combine[:, rows] * step,
            back,
            preferred_element_type=F32,
            precision=lax.Precision.HIGHEST,
        )
    for q in range(nq):
        for h in range(2):
            fin_send[2 * q + h] = mixed[
                q * t_rows : (q + 1) * t_rows, h * part : (h + 1) * part
            ]
    for d in far_rows:
        y = turn(row, d, n_row)
        remote(
            fin_send.at[y], fin_recv.at[d - 1], fi_s, fi_r, me, y * CORES + core
        ).start()
    remote(fin_recv, fin_recv, fi_s, fi_r, me, tp).wait_recv()
    total += fin_send[row]
    for d in range(1, n_row):
        total += fin_recv[d - 1]
    eye = lax.broadcasted_iota(jnp.int32, (t_rows, 128), 0) == lax.broadcasted_iota(
        jnp.int32, (t_rows, 128), 1
    )
    mine_sq = jnp.sum(
        jnp.where(eye, jnp.sum(total * total, axis=1, keepdims=True), 0.0),
        axis=0,
        keepdims=True,
    )
    sq_send[...] = mine_sq
    for d in far_tp:
        remote(sq_send, sq_recv.at[d - 1], sq_s, sq_r, me, turn(tp, d, n_tp)).start()
    remote(sq_recv, sq_recv, sq_s, sq_r, me, tp).wait_recv()
    all_sq = mine_sq
    for d in range(1, n_tp):
        all_sq += sq_recv[d - 1]
    all_sq = jnp.sum(jnp.where(eye, all_sq, 0.0), axis=1, keepdims=True)
    scale = lax.rsqrt(all_sq / width + norm_eps)
    out_ref[...] = (total * scale * og[...]).astype(out_ref.dtype)
    at = pl.ds(0, n_tp - 1)
    remote(tok.at[at], tok.at[at], ag_s, ag_r, me, tp).wait_send()
    remote(dense_recv.at[at], dense_recv.at[at], de_s, de_r, me, tp).wait_send()
    remote(sq_recv, sq_recv, sq_s, sq_r, me, tp).wait_send()
    at = pl.ds(0, n_ep - 1)
    remote(disp_send.at[at], disp_send.at[at], di_s, di_r.at[0], me, tp).wait_send()
    remote(scl_send.at[at], scl_recv.at[at], sc_s, sc_r.at[0], me, tp).wait_send()
    at = pl.ds(0, (n_ep - 1) * big)
    remote(ret_send.at[at], ret_recv.at[at], re_s, re_r.at[0], me, tp).wait_send()
    spot = grid.at[0, pl.ds(0, n_row - 1)]
    remote(spot, spot, ya_s, ya_r.at[0], me, tp).wait_send()
    remote(grid.at[0], grid.at[0], pf_s, pf_r.at[0], me, tp).wait_send()
    remote(pair_send, pair_recv, pa_s, pa_r.at[0], me, tp).wait_send()
    remote(fin_recv, fin_recv, fi_s, fi_r, me, tp).wait_send()


def shards(n_ep, n_tp, *args):
    (tok, gain, route, logit, eg, eu, ed, dg, du, dd, mixw, og) = args
    t_rows, part = tok.shape
    width = part * n_tp
    half = part // 2
    n_loc, _, ff = eg.shape
    ffd = dg.shape[1]
    hid = n_loc * ff
    n_row = n_tp // CORES
    slot = n_loc * CAP
    blk = 2 * slot
    nq = n_row // 2
    big = n_ep * nq * slot
    wide = 2 * part
    n_chunk = chunks_of(n_ep)
    dma = pltpu.SemaphoreType.DMA
    V = pltpu.VMEM
    scratch = [
        V((n_tp, t_rows, part), BF16),
        V((1, width), F32),
        V(route.shape[::-1], jnp.int32),
        V(logit.shape[::-1], F32),
        V((2 * hid, width), BF16),
        V((hid, width), BF16),
        V((CORES, nq * hid, wide), BF16),
        V((2 * ffd, width), BF16),
        V(dd.shape, BF16),
        V((1, width), F32),
        V((1, part), F32),
        V((t_rows, width), BF16),
        V((n_ep, blk, half), BF16),
        V((CORES, n_row, n_ep, blk, half), BF16),
        V((n_ep * slot, width), BF16),
        V((big, nq * hid), BF16),
        V((n_tp, t_rows, part), F32),
        V((n_tp - 1, t_rows, part), F32),
        V((big, wide), F32),
        V((big, wide), F32),
        V((big, wide), jnp.int16),
        V((big, wide), jnp.int16),
        V((n_ep, 1, 128), F32),
        V((n_ep, 1, 128), F32),
        V((n_row, t_rows, part), F32),
        V((n_row - 1, t_rows, part), F32),
        V((1, 128), F32),
        V((n_tp - 1, 1, 128), F32),
        dma((12,)),
        dma,
        dma,
        dma,
        dma((n_chunk,)),
        dma,
        dma((n_chunk,)),
        dma,
        dma((n_chunk,)),
        dma,
        dma,
        dma,
        dma((n_chunk,)),
        dma,
        dma((n_chunk,)),
        dma,
        dma((n_chunk,)),
        dma,
        dma,
        dma,
        dma,
    ]
    return pl.pallas_call(
        functools.partial(kernel, n_ep, n_tp, n_loc),
        out_shape=jax.ShapeDtypeStruct((t_rows, part), BF16),
        in_specs=[pl.BlockSpec(memory_space=pltpu.HBM)] * 12,
        out_specs=pl.BlockSpec(memory_space=pltpu.VMEM),
        scratch_shapes=scratch,
        compiler_params=pltpu.CompilerParams(
            collective_id=0, has_side_effects=True, vmem_limit_bytes=60 * 1024 * 1024
        ),
        name="moe_layer",
    )(
        tok,
        gain.reshape(1, width),
        route.T,
        logit.T,
        eg.swapaxes(1, 2).reshape(hid, width),
        eu.swapaxes(1, 2).reshape(hid, width),
        ed.reshape(hid, width),
        dg.T,
        du.T,
        dd,
        mixw.reshape(1, width),
        og.reshape(1, part),
    )


def solution(mesh):
    placed = (
        P("ep", "tp"),
        P(),
        P("ep", None),
        P("ep", None),
        P("ep", None, "tp"),
        P("ep", None, "tp"),
        P("ep", "tp", None),
        P(None, "tp"),
        P(None, "tp"),
        P("tp", None),
        P(),
        P("tp"),
    )
    return jax.shard_map(
        functools.partial(shards, mesh.shape["ep"], mesh.shape["tp"]),
        mesh=mesh,
        in_specs=placed,
        out_specs=P("ep", "tp"),
        check_vma=False,
    )
```

```python
import functools

import jax
import jax.numpy as jnp
from jax import lax
from jax.experimental import pallas as pl
from jax.experimental.pallas import tpu as pltpu
from jax.sharding import PartitionSpec as P

CAP = 2
CORES = 2
NX = 4
CHUNKS = 4
norm_eps = 1e-06
MESH = pl.DeviceIdType.MESH
F32 = jnp.float32
BF16 = jnp.bfloat16
NT = (((1,), (1,)), ((), ()))


def silu(v):
    return v / (1.0 + jnp.exp(-v))


def chunks_of(n_ep):
    return CHUNKS if n_ep >= 2 * CHUNKS else 2


def paired(i, n):
    h = n // 2 - 1 - i // 2
    if i < n - 2:
        return h if i % 2 == 0 else n - h
    return n // 2 if i == n - 2 else 0


def paired_vec(i, n):
    h = n // 2 - 1 - (i >> 1)
    return jnp.where(
        i < n - 2,
        jnp.where((i & 1) == 0, h, n - h),
        jnp.where(i == n - 2, n // 2, 0),
    )


def kernel(
    n_ep,
    n_tp,
    n_loc,
    tok_hbm,
    gain_hbm,
    route_hbm,
    logit_hbm,
    eg_hbm,
    eu_hbm,
    ed_hbm,
    dg_hbm,
    du_hbm,
    dd_hbm,
    mix_hbm,
    og_hbm,
    out_ref,
    tok,
    gain,
    route,
    logit,
    wgu,
    ednat,
    ed,
    wd,
    dd,
    mixw,
    og,
    normed,
    disp_send,
    grid,
    rows_n,
    hid4,
    dense_send,
    dense_recv,
    pair_send,
    pair_recv,
    ret_send,
    ret_recv,
    scl_send,
    scl_recv,
    fin_send,
    fin_recv,
    sq_send,
    sq_recv,
    lsem,
    ag_s,
    ag_r,
    di_s,
    di_r,
    ya_s,
    ya_r,
    pf_s,
    pf_r,
    de_s,
    de_r,
    pa_s,
    pa_r,
    re_s,
    re_r,
    sc_s,
    sc_r,
    fi_s,
    fi_r,
    sq_s,
    sq_r,
):
    me = lax.axis_index("ep")
    tp = lax.axis_index("tp")
    core = lax.rem(tp, CORES)
    row = lax.div(tp, CORES)
    n_row = n_tp // CORES
    partner = row * CORES + (1 - core)
    t_rows, part = tok.shape[1], tok.shape[2]
    width = part * n_tp
    half = part // 2
    nx = min(NX, n_ep)
    nz = n_ep // nx
    my_z = lax.div(me, nx)
    my_x = lax.rem(me, nx)
    slot = n_loc * CAP
    blk = 2 * slot
    slots = n_ep * blk
    keys = 2 * t_rows
    hid = ednat.shape[0]
    n_chunk = chunks_of(n_ep)
    order = [0, 3, 1, 2]
    per = n_ep // n_chunk
    crow = per * blk
    xrow = per * slot
    nq = n_row // 2
    big = nq * slot
    brow = per * big
    wide = 2 * part
    far_rows = sorted(range(1, n_row), key=lambda d: -min(d, n_row - d))
    far_tp = sorted(range(1, n_tp), key=lambda d: -min(d, n_tp - d))

    def turn(base, d, n):
        return lax.rem(base + d, n)

    def remote(src, dst, s, r, e, t):
        return pltpu.make_async_remote_copy(
            src_ref=src,
            dst_ref=dst,
            send_sem=s,
            recv_sem=r,
            device_id={"ep": e, "tp": t},
            device_id_type=MESH,
        )

    def offsets(b):
        return paired(b // nx, nz), paired(b % nx, nx)

    def ahead(b):
        dz, dx = offsets(b)
        return turn(my_z, dz, nz) * nx + turn(my_x, dx, nx)

    def behind(b):
        dz, dx = offsets(b)
        return turn(my_z, (nz - dz) % nz, nz) * nx + turn(my_x, (nx - dx) % nx, nx)

    def chunk(c):
        return pl.ds(c * per, per)

    half_w = wgu.shape[0] // 2
    ffd = wd.shape[0] // 2
    loads = []
    pairs = [
        (tok_hbm, tok.at[tp]),
        (route_hbm, route),
        (logit_hbm, logit),
        (gain_hbm, gain),
        (mix_hbm, mixw),
        (og_hbm, og),
        (dg_hbm, wd.at[0:ffd]),
        (du_hbm, wd.at[ffd : 2 * ffd]),
        (dd_hbm, dd),
        (ed_hbm, ednat),
        (eg_hbm, wgu.at[0:half_w]),
        (eu_hbm, wgu.at[half_w : 2 * half_w]),
    ]
    for i, (src, dst) in enumerate(pairs):
        loads.append(pltpu.make_async_copy(src, dst, lsem.at[i]))
    for c in loads[0:2]:
        c.start()
    barrier = pltpu.get_barrier_semaphore()
    greeted = 0
    for j in range(n_ep - 1):
        pl.semaphore_signal(
            barrier, inc=1, device_id={"ep": ahead(j), "tp": tp}, device_id_type=MESH
        )
        greeted += 1
    for d in far_tp:
        pl.semaphore_signal(
            barrier, inc=1, device_id={"ep": me, "tp": turn(tp, d, n_tp)}, device_id_type=MESH
        )
        greeted += 1
    for c in loads[2:]:
        c.start()

    loads[1].wait()
    spread = (
        lax.broadcasted_iota(jnp.int32, (t_rows, keys), 0)
        == (lax.broadcasted_iota(jnp.int32, (t_rows, keys), 1) % t_rows)
    ).astype(F32)
    both = jnp.dot(route[...].astype(F32), spread, preferred_element_type=F32)
    ri = lax.broadcasted_iota(jnp.int32, (keys, keys), 0)
    ci = lax.broadcasted_iota(jnp.int32, (keys, keys), 1)
    tri = ((ri < ci) & ((ri // t_rows) == (ci // t_rows))).astype(F32)
    r = lax.broadcasted_iota(jnp.int32, (slots, keys), 0)
    k = lax.broadcasted_iota(jnp.int32, (slots, keys), 1)
    b = r // blk
    s = r % slot
    dz = paired_vec(b // nx, nz)
    dx = paired_vec(b % nx, nx)
    dest = ((my_z + dz) & (nz - 1)) * nx + ((my_x + dx) & (nx - 1))
    slot_e = (dest * n_loc + s // CAP).astype(F32)
    same = ((r // slot) % 2) == (k // t_rows)
    hit0 = (slot_e == both[0:1, :]).astype(F32)
    hit1 = (slot_e == both[1:2, :]).astype(F32)
    hits = hit0 + hit1
    before = jnp.dot(hits, tri, preferred_element_type=F32)
    place = jnp.where(same & (before == (s % CAP).astype(F32)), hits, 0.0)
    loads[0].wait()
    x = tok[tp].astype(F32)
    source = jnp.concatenate([x[:, 0:half], x[:, half:part]], axis=0).astype(BF16)
    placed = jnp.dot(place.astype(BF16), source, preferred_element_type=F32)
    placed = placed.reshape(n_ep, blk, half).astype(BF16)
    disp_send[...] = placed
    pl.semaphore_wait(barrier, greeted)
    for j in range(n_ep - 1):
        remote(
            disp_send.at[j], grid.at[core, row, j], di_s, di_r.at[j // per], ahead(j), tp
        ).start()
    for d in far_tp:
        remote(tok.at[tp], tok.at[tp], ag_s, ag_r, me, turn(tp, d, n_tp)).start()
    grid[core, row, n_ep - 1] = placed[n_ep - 1]

    loads[2].wait()
    l0 = logit[0:1, :]
    l1 = logit[1:2, :]
    top = jnp.maximum(l0, l1)
    e0 = jnp.exp(l0 - top)
    e1 = jnp.exp(l1 - top)
    shares = jnp.concatenate([e0 / (e0 + e1), e1 / (e0 + e1)], axis=0)
    names = jnp.concatenate([route[...].astype(F32), shares], axis=0)
    bkeys = nq * t_rows
    bspread = (
        lax.broadcasted_iota(jnp.int32, (t_rows, bkeys), 0)
        == (lax.broadcasted_iota(jnp.int32, (t_rows, bkeys), 1) % t_rows)
    ).astype(F32)
    names = jnp.dot(
        names, bspread, preferred_element_type=F32, precision=lax.Precision.HIGHEST
    )
    ri = lax.broadcasted_iota(jnp.int32, (bkeys, bkeys), 0)
    ci = lax.broadcasted_iota(jnp.int32, (bkeys, bkeys), 1)
    tri = ((ri < ci) & ((ri // t_rows) == (ci // t_rows))).astype(F32)
    r = lax.broadcasted_iota(jnp.int32, (n_ep * big, bkeys), 0)
    k = lax.broadcasted_iota(jnp.int32, (n_ep * big, bkeys), 1)
    b = r // big
    s = r % slot
    dz = paired_vec(b // nx, nz)
    dx = paired_vec(b % nx, nx)
    dest = ((my_z + dz) & (nz - 1)) * nx + ((my_x + dx) & (nx - 1))
    slot_e = (dest * n_loc + s // CAP).astype(F32)
    same = ((r // slot) % nq) == (k // t_rows)
    hit0 = (slot_e == names[0:1, :]).astype(F32)
    hit1 = (slot_e == names[1:2, :]).astype(F32)
    before = jnp.dot(hit0 + hit1, tri, preferred_element_type=F32)
    taken = same & (before == (s % CAP).astype(F32))
    combine = jnp.where(taken, hit0 * names[2:3, :] + hit1 * names[3:4, :], 0.0).T
    pr = lax.broadcasted_iota(jnp.int32, (crow, crow), 0)
    pc = lax.broadcasted_iota(jnp.int32, (crow, crow), 1)
    perm = (
        ((pr // xrow) == ((pc // slot) % 2))
        & (((pr // slot) % per) == (pc // blk))
        & ((pr % slot) == (pc % slot))
    ).astype(BF16)
    xr = lax.broadcasted_iota(jnp.int32, (brow, xrow), 0)
    xc = lax.broadcasted_iota(jnp.int32, (brow, xrow), 1)
    expand = (((xr // big) == (xc // slot)) & ((xr % slot) == (xc % slot))).astype(BF16)
    sr = lax.broadcasted_iota(jnp.int32, (brow, 128), 0)
    sc = lax.broadcasted_iota(jnp.int32, (brow, 128), 1)
    in_lane = (sr % big) == sc
    gr = lax.broadcasted_iota(jnp.int32, (per, brow), 0)
    gc = lax.broadcasted_iota(jnp.int32, (per, brow), 1)
    in_block = gr == (gc // big)
    br = lax.broadcasted_iota(jnp.int32, (128, brow), 0)
    bc = lax.broadcasted_iota(jnp.int32, (128, brow), 1)
    unlane = (br == (bc % big)).astype(BF16)
    loads[9].wait()
    for g in range(CORES):
        for q in range(nq):
            for h in range(2):
                at = (CORES * (2 * q + h) + g) * part
                ed[g, q * hid : (q + 1) * hid, h * part : (h + 1) * part] = ednat[
                    :, at : at + part
                ]

    for c in order:
        at = pl.ds(c * per, per - (c == n_chunk - 1))
        remote(
            disp_send.at[at], grid.at[core, row, at], di_s, di_r.at[c], me, tp
        ).wait_recv()
        for d in far_rows:
            spot = grid.at[core, row, chunk(c)]
            remote(spot, spot, ya_s, ya_r.at[c], me, turn(row, d, n_row) * CORES + core).start()

    for i in (3, 4, 5):
        loads[i].wait()
    at = pl.ds(0, n_tp - 1)
    remote(tok.at[at], tok.at[at], ag_s, ag_r, me, tp).wait_recv()
    squares = jnp.zeros((t_rows, part), F32)
    for t in range(n_tp):
        x = tok[t].astype(F32)
        squares += x * x
    inv = lax.rsqrt(jnp.sum(squares, axis=1, keepdims=True) / width + norm_eps)
    mix = jnp.zeros((t_rows, part), F32)
    for t in range(n_tp):
        cols = slice(t * part, (t + 1) * part)
        nt = (tok[t].astype(F32) * inv * gain[:, cols]).astype(BF16)
        normed[:, cols] = nt
        mix += nt.astype(F32) * mixw[:, cols]
    mix_gate = 1.0 / (1.0 + jnp.exp(-jnp.sum(mix, axis=1, keepdims=True)))
    for i in (6, 7, 8):
        loads[i].wait()
    both = lax.dot_general(normed[...], wd[...], NT, preferred_element_type=F32)
    dh = (silu(both[:, 0:ffd]) * both[:, ffd : 2 * ffd]).astype(BF16)
    for t in range(n_tp):
        dense_send[t] = jnp.dot(
            dh, dd[:, t * part : (t + 1) * part], preferred_element_type=F32
        )
    for d in far_tp:
        t = turn(tp, d, n_tp)
        remote(dense_send.at[t], dense_recv.at[d - 1], de_s, de_r, me, t).start()
    for i in (10, 11):
        loads[i].wait()

    def unpack(c, g):
        slabs = [
            grid[g, y, c * per : (c + 1) * per].astype(F32).reshape(crow, half)
            for y in range(n_row)
        ]
        moved = jnp.dot(
            perm, jnp.concatenate(slabs, axis=1).astype(BF16), preferred_element_type=F32
        )
        total = jnp.zeros((xrow, half), F32)
        for y in range(n_row):
            for h in range(2):
                v = moved[h * xrow : (h + 1) * xrow, y * half : (y + 1) * half]
                at = pl.multiple_of((CORES * y + g) * part + h * half, half)
                rows_n[c * xrow : (c + 1) * xrow, pl.ds(at, half)] = v.astype(BF16)
                total += v * v
        return jnp.sum(total, axis=1, keepdims=True)

    ar = lax.broadcasted_iota(jnp.int32, (xrow, hid), 0)
    ac = lax.broadcasted_iota(jnp.int32, (xrow, hid), 1)
    mine = ((ar % slot) // CAP) == (ac // (hid // n_loc))
    hr = lax.broadcasted_iota(jnp.int32, (brow, hid), 0)
    seen = {}

    def gather(c):
        at = pl.ds(0, n_row - 1)
        spot = grid.at[core, at, chunk(c)]
        remote(spot, spot, ya_s, ya_r.at[c], me, tp).wait_recv()
        spot = grid.at[core, :, chunk(c)]
        remote(spot, spot, pf_s, pf_r.at[c], me, partner).start()
        seen[c] = unpack(c, core)

    def apply(c):
        spot = grid.at[1 - core, :, chunk(c)]
        remote(spot, spot, pf_s, pf_r.at[c], me, tp).wait_recv()
        inv = lax.rsqrt((seen[c] + unpack(c, 1 - core)) / width + norm_eps)
        rows = slice(c * xrow, (c + 1) * xrow)
        for t in range(n_tp):
            cols = slice(t * part, (t + 1) * part)
            rows_n[rows, cols] = (rows_n[rows, cols].astype(F32) * inv * gain[:, cols]).astype(
                BF16
            )
        act = lax.dot_general(rows_n[rows, :], wgu[...], NT, preferred_element_type=F32)
        hidden = jnp.where(mine, silu(act[:, 0:hid]) * act[:, hid : 2 * hid], 0.0)
        wider = jnp.dot(expand, hidden.astype(BF16), preferred_element_type=F32)
        rows = slice(c * brow, (c + 1) * brow)
        for q in range(nq):
            hid4[rows, q * hid : (q + 1) * hid] = jnp.where(
                ((hr // slot) % nq) == q, wider, 0.0
            ).astype(BF16)
        pair_send[rows, :] = jnp.dot(hid4[rows, :], ed[1 - core], preferred_element_type=F32)
        at = pl.ds(c * brow, brow)
        remote(pair_send.at[at], pair_recv.at[at], pa_s, pa_r.at[c], me, partner).start()

    def reply(c):
        rows = slice(c * brow, (c + 1) * brow)
        v = jnp.dot(hid4[rows, :], ed[core], preferred_element_type=F32)
        at = pl.ds(c * brow, brow)
        remote(pair_send.at[at], pair_recv.at[at], pa_s, pa_r.at[c], me, tp).wait_recv()
        v = v + pair_recv[rows, :]
        peak = jnp.max(jnp.abs(v), axis=1, keepdims=True)
        step = (jnp.maximum(peak, 1e-30) * (1.0 / 32600.0)).astype(BF16).astype(F32)
        ret_send[rows, :] = (
            jnp.floor(v * (1.0 / step) + 0.5).astype(jnp.int32).astype(jnp.int16)
        )
        lanes = jnp.where(in_lane, step, 0.0).astype(BF16)
        steps = jnp.dot(in_block.astype(BF16), lanes, preferred_element_type=F32)
        for i in range(per):
            j = c * per + i
            scl_send[j] = steps[i : i + 1, :]
            if j < n_ep - 1:
                at = pl.ds(j * big, big)
                remote(
                    ret_send.at[at], ret_recv.at[at], re_s, re_r.at[c], behind(j), tp
                ).start()
                remote(
                    scl_send.at[j], scl_recv.at[j], sc_s, sc_r.at[c], behind(j), tp
                ).start()
        if c == n_chunk - 1:
            tail = slice((n_ep - 1) * big, n_ep * big)
            ret_recv[tail, :] = ret_send[tail, :]
            scl_recv[n_ep - 1] = scl_send[n_ep - 1]

    for i, c in enumerate(order):
        gather(c)
        if i > 0:
            reply(order[i - 1])
        apply(c)
    reply(order[-1])
    at = pl.ds(0, n_tp - 1)
    remote(dense_recv.at[at], dense_recv.at[at], de_s, de_r, me, tp).wait_recv()
    total = dense_send[tp]
    for d in range(1, n_tp):
        total += dense_recv[d - 1]
    total = mix_gate * total
    mixed = jnp.zeros((bkeys, wide), F32)
    for c in order:
        n = per - (c == n_chunk - 1)
        at = pl.ds(c * brow, n * big)
        remote(ret_send.at[at], ret_recv.at[at], re_s, re_r.at[c], me, tp).wait_recv()
        at = pl.ds(c * per, n)
        remote(scl_send.at[at], scl_recv.at[at], sc_s, sc_r.at[c], me, tp).wait_recv()
        rows = slice(c * brow, (c + 1) * brow)
        steps = jnp.concatenate([scl_recv[c * per + i] for i in range(per)], axis=0)
        lanes = jnp.dot(steps.astype(BF16), unlane, preferred_element_type=F32)
        step = jnp.sum(jnp.where(in_block, lanes, 0.0), axis=0, keepdims=True)
        back = ret_recv[rows, :].astype(jnp.int32).astype(F32)
        mixed += jnp.dot(
            combine[:, rows] * step,
            back,
            preferred_element_type=F32,
            precision=lax.Precision.HIGHEST,
        )
    for q in range(nq):
        for h in range(2):
            fin_send[2 * q + h] = mixed[
                q * t_rows : (q + 1) * t_rows, h * part : (h + 1) * part
            ]
    for d in far_rows:
        y = turn(row, d, n_row)
        remote(
            fin_send.at[y], fin_recv.at[d - 1], fi_s, fi_r, me, y * CORES + core
        ).start()
    remote(fin_recv, fin_recv, fi_s, fi_r, me, tp).wait_recv()
    total += fin_send[row]
    for d in range(1, n_row):
        total += fin_recv[d - 1]
    eye = lax.broadcasted_iota(jnp.int32, (t_rows, 128), 0) == lax.broadcasted_iota(
        jnp.int32, (t_rows, 128), 1
    )
    mine_sq = jnp.sum(
        jnp.where(eye, jnp.sum(total * total, axis=1, keepdims=True), 0.0),
        axis=0,
        keepdims=True,
    )
    sq_send[...] = mine_sq
    for d in far_tp:
        remote(sq_send, sq_recv.at[d - 1], sq_s, sq_r, me, turn(tp, d, n_tp)).start()
    remote(sq_recv, sq_recv, sq_s, sq_r, me, tp).wait_recv()
    all_sq = mine_sq
    for d in range(1, n_tp):
        all_sq += sq_recv[d - 1]
    all_sq = jnp.sum(jnp.where(eye, all_sq, 0.0), axis=1, keepdims=True)
    scale = lax.rsqrt(all_sq / width + norm_eps)
    out_ref[...] = (total * scale * og[...]).astype(out_ref.dtype)
    at = pl.ds(0, n_tp - 1)
    remote(tok.at[at], tok.at[at], ag_s, ag_r, me, tp).wait_send()
    remote(dense_recv.at[at], dense_recv.at[at], de_s, de_r, me, tp).wait_send()
    remote(sq_recv, sq_recv, sq_s, sq_r, me, tp).wait_send()
    at = pl.ds(0, n_ep - 1)
    remote(disp_send.at[at], disp_send.at[at], di_s, di_r.at[0], me, tp).wait_send()
    remote(scl_send.at[at], scl_recv.at[at], sc_s, sc_r.at[0], me, tp).wait_send()
    at = pl.ds(0, (n_ep - 1) * big)
    remote(ret_send.at[at], ret_recv.at[at], re_s, re_r.at[0], me, tp).wait_send()
    spot = grid.at[0, pl.ds(0, n_row - 1)]
    remote(spot, spot, ya_s, ya_r.at[0], me, tp).wait_send()
    remote(grid.at[0], grid.at[0], pf_s, pf_r.at[0], me, tp).wait_send()
    remote(pair_send, pair_recv, pa_s, pa_r.at[0], me, tp).wait_send()
    remote(fin_recv, fin_recv, fi_s, fi_r, me, tp).wait_send()


def shards(n_ep, n_tp, *args):
    (tok, gain, route, logit, eg, eu, ed, dg, du, dd, mixw, og) = args
    t_rows, part = tok.shape
    width = part * n_tp
    half = part // 2
    n_loc, _, ff = eg.shape
    ffd = dg.shape[1]
    hid = n_loc * ff
    n_row = n_tp // CORES
    slot = n_loc * CAP
    blk = 2 * slot
    nq = n_row // 2
    big = n_ep * nq * slot
    wide = 2 * part
    n_chunk = chunks_of(n_ep)
    dma = pltpu.SemaphoreType.DMA
    V = pltpu.VMEM
    scratch = [
        V((n_tp, t_rows, part), BF16),
        V((1, width), F32),
        V(route.shape[::-1], jnp.int32),
        V(logit.shape[::-1], F32),
        V((2 * hid, width), BF16),
        V((hid, width), BF16),
        V((CORES, nq * hid, wide), BF16),
        V((2 * ffd, width), BF16),
        V(dd.shape, BF16),
        V((1, width), F32),
        V((1, part), F32),
        V((t_rows, width), BF16),
        V((n_ep, blk, half), BF16),
        V((CORES, n_row, n_ep, blk, half), BF16),
        V((n_ep * slot, width), BF16),
        V((big, nq * hid), BF16),
        V((n_tp, t_rows, part), F32),
        V((n_tp - 1, t_rows, part), F32),
        V((big, wide), F32),
        V((big, wide), F32),
        V((big, wide), jnp.int16),
        V((big, wide), jnp.int16),
        V((n_ep, 1, 128), F32),
        V((n_ep, 1, 128), F32),
        V((n_row, t_rows, part), F32),
        V((n_row - 1, t_rows, part), F32),
        V((1, 128), F32),
        V((n_tp - 1, 1, 128), F32),
        dma((12,)),
        dma,
        dma,
        dma,
        dma((n_chunk,)),
        dma,
        dma((n_chunk,)),
        dma,
        dma((n_chunk,)),
        dma,
        dma,
        dma,
        dma((n_chunk,)),
        dma,
        dma((n_chunk,)),
        dma,
        dma((n_chunk,)),
        dma,
        dma,
        dma,
        dma,
    ]
    return pl.pallas_call(
        functools.partial(kernel, n_ep, n_tp, n_loc),
        out_shape=jax.ShapeDtypeStruct((t_rows, part), BF16),
        in_specs=[pl.BlockSpec(memory_space=pltpu.HBM)] * 12,
        out_specs=pl.BlockSpec(memory_space=pltpu.VMEM),
        scratch_shapes=scratch,
        compiler_params=pltpu.CompilerParams(
            collective_id=0, has_side_effects=True, vmem_limit_bytes=60 * 1024 * 1024
        ),
        name="moe_layer",
    )(
        tok,
        gain.reshape(1, width),
        route.T,
        logit.T,
        eg.swapaxes(1, 2).reshape(hid, width),
        eu.swapaxes(1, 2).reshape(hid, width),
        ed.reshape(hid, width),
        dg.T,
        du.T,
        dd,
        mixw.reshape(1, width),
        og.reshape(1, part),
    )


def solution(mesh):
    placed = (
        P("ep", "tp"),
        P(),
        P("ep", None),
        P("ep", None),
        P("ep", None, "tp"),
        P("ep", None, "tp"),
        P("ep", "tp", None),
        P(None, "tp"),
        P(None, "tp"),
        P("tp", None),
        P(),
        P("tp"),
    )
    return jax.shard_map(
        functools.partial(shards, mesh.shape["ep"], mesh.shape["tp"]),
        mesh=mesh,
        in_specs=placed,
        out_specs=P("ep", "tp"),
        check_vma=False,
    )
```

```python
import functools

import jax
import jax.numpy as jnp
from jax import lax
from jax.experimental import pallas as pl
from jax.experimental.pallas import tpu as pltpu
from jax.sharding import PartitionSpec as P

CAP = 2
CORES = 2
NX = 4
CHUNKS = 4
norm_eps = 1e-06
MESH = pl.DeviceIdType.MESH
F32 = jnp.float32
BF16 = jnp.bfloat16
NT = (((1,), (1,)), ((), ()))


def silu(v):
    return v / (1.0 + jnp.exp(-v))


def chunks_of(n_ep):
    return CHUNKS if n_ep >= 2 * CHUNKS else 2


def paired(i, n):
    h = n // 2 - 1 - i // 2
    if i < n - 2:
        return h if i % 2 == 0 else n - h
    return n // 2 if i == n - 2 else 0


def paired_vec(i, n):
    h = n // 2 - 1 - (i >> 1)
    return jnp.where(
        i < n - 2,
        jnp.where((i & 1) == 0, h, n - h),
        jnp.where(i == n - 2, n // 2, 0),
    )


def kernel(
    n_ep,
    n_tp,
    n_loc,
    tok_hbm,
    gain_hbm,
    route_hbm,
    logit_hbm,
    eg_hbm,
    eu_hbm,
    ed_hbm,
    dg_hbm,
    du_hbm,
    dd_hbm,
    mix_hbm,
    og_hbm,
    out_ref,
    tok,
    gain,
    route,
    logit,
    wgu,
    ednat,
    ed,
    wd,
    dd,
    mixw,
    og,
    normed,
    disp_send,
    grid,
    rows_n,
    hid4,
    dense_send,
    dense_recv,
    pair_send,
    pair_recv,
    ret_send,
    ret_recv,
    scl_send,
    scl_recv,
    fin_send,
    fin_recv,
    sq_send,
    sq_recv,
    lsem,
    ag_s,
    ag_r,
    di_s,
    di_r,
    ya_s,
    ya_r,
    pf_s,
    pf_r,
    de_s,
    de_r,
    pa_s,
    pa_r,
    re_s,
    re_r,
    sc_s,
    sc_r,
    fi_s,
    fi_r,
    sq_s,
    sq_r,
):
    me = lax.axis_index("ep")
    tp = lax.axis_index("tp")
    core = lax.rem(tp, CORES)
    row = lax.div(tp, CORES)
    n_row = n_tp // CORES
    partner = row * CORES + (1 - core)
    t_rows, part = tok.shape[1], tok.shape[2]
    width = part * n_tp
    half = part // 2
    nx = min(NX, n_ep)
    nz = n_ep // nx
    my_z = lax.div(me, nx)
    my_x = lax.rem(me, nx)
    slot = n_loc * CAP
    blk = 2 * slot
    slots = n_ep * blk
    keys = 2 * t_rows
    hid = ednat.shape[0]
    n_chunk = chunks_of(n_ep)
    order = [0, 3, 1, 2]
    per = n_ep // n_chunk
    crow = per * blk
    xrow = per * slot
    nq = n_row // 2
    big = nq * slot
    brow = per * big
    wide = 2 * part
    far_rows = sorted(range(1, n_row), key=lambda d: -min(d, n_row - d))
    far_tp = sorted(range(1, n_tp), key=lambda d: -min(d, n_tp - d))

    def turn(base, d, n):
        return lax.rem(base + d, n)

    def remote(src, dst, s, r, e, t):
        return pltpu.make_async_remote_copy(
            src_ref=src,
            dst_ref=dst,
            send_sem=s,
            recv_sem=r,
            device_id={"ep": e, "tp": t},
            device_id_type=MESH,
        )

    def offsets(b):
        return paired(b // nx, nz), paired(b % nx, nx)

    def ahead(b):
        dz, dx = offsets(b)
        return turn(my_z, dz, nz) * nx + turn(my_x, dx, nx)

    def behind(b):
        dz, dx = offsets(b)
        return turn(my_z, (nz - dz) % nz, nz) * nx + turn(my_x, (nx - dx) % nx, nx)

    def chunk(c):
        return pl.ds(c * per, per)

    half_w = wgu.shape[0] // 2
    ffd = wd.shape[0] // 2
    loads = []
    pairs = [
        (tok_hbm, tok.at[tp]),
        (route_hbm, route),
        (logit_hbm, logit),
        (gain_hbm, gain),
        (mix_hbm, mixw),
        (og_hbm, og),
        (dg_hbm, wd.at[0:ffd]),
        (du_hbm, wd.at[ffd : 2 * ffd]),
        (dd_hbm, dd),
        (ed_hbm, ednat),
        (eg_hbm, wgu.at[0:half_w]),
        (eu_hbm, wgu.at[half_w : 2 * half_w]),
    ]
    for i, (src, dst) in enumerate(pairs):
        loads.append(pltpu.make_async_copy(src, dst, lsem.at[i]))
    for c in loads[0:2]:
        c.start()
    barrier = pltpu.get_barrier_semaphore()
    greeted = 0
    for j in range(n_ep - 1):
        pl.semaphore_signal(
            barrier, inc=1, device_id={"ep": ahead(j), "tp": tp}, device_id_type=MESH
        )
        greeted += 1
    for d in far_tp:
        pl.semaphore_signal(
            barrier, inc=1, device_id={"ep": me, "tp": turn(tp, d, n_tp)}, device_id_type=MESH
        )
        greeted += 1
    for c in loads[2:]:
        c.start()

    loads[1].wait()
    spread = (
        lax.broadcasted_iota(jnp.int32, (t_rows, keys), 0)
        == (lax.broadcasted_iota(jnp.int32, (t_rows, keys), 1) % t_rows)
    ).astype(F32)
    both = jnp.dot(route[...].astype(F32), spread, preferred_element_type=F32)
    ri = lax.broadcasted_iota(jnp.int32, (keys, keys), 0)
    ci = lax.broadcasted_iota(jnp.int32, (keys, keys), 1)
    tri = ((ri < ci) & ((ri // t_rows) == (ci // t_rows))).astype(F32)
    r = lax.broadcasted_iota(jnp.int32, (slots, keys), 0)
    k = lax.broadcasted_iota(jnp.int32, (slots, keys), 1)
    b = r // blk
    s = r % slot
    dz = paired_vec(b // nx, nz)
    dx = paired_vec(b % nx, nx)
    dest = ((my_z + dz) & (nz - 1)) * nx + ((my_x + dx) & (nx - 1))
    slot_e = (dest * n_loc + s // CAP).astype(F32)
    same = ((r // slot) % 2) == (k // t_rows)
    hit0 = (slot_e == both[0:1, :]).astype(F32)
    hit1 = (slot_e == both[1:2, :]).astype(F32)
    hits = hit0 + hit1
    before = jnp.dot(hits, tri, preferred_element_type=F32)
    place = jnp.where(same & (before == (s % CAP).astype(F32)), hits, 0.0)
    loads[0].wait()
    x = tok[tp].astype(F32)
    source = jnp.concatenate([x[:, 0:half], x[:, half:part]], axis=0).astype(BF16)
    placed = jnp.dot(place.astype(BF16), source, preferred_element_type=F32)
    placed = placed.reshape(n_ep, blk, half).astype(BF16)
    disp_send[...] = placed
    pl.semaphore_wait(barrier, greeted)
    for j in range(n_ep - 1):
        remote(
            disp_send.at[j], grid.at[core, row, j], di_s, di_r.at[j // per], ahead(j), tp
        ).start()
    for d in far_tp:
        remote(tok.at[tp], tok.at[tp], ag_s, ag_r, me, turn(tp, d, n_tp)).start()
    grid[core, row, n_ep - 1] = placed[n_ep - 1]

    loads[2].wait()
    l0 = logit[0:1, :]
    l1 = logit[1:2, :]
    top = jnp.maximum(l0, l1)
    e0 = jnp.exp(l0 - top)
    e1 = jnp.exp(l1 - top)
    shares = jnp.concatenate([e0 / (e0 + e1), e1 / (e0 + e1)], axis=0)
    names = jnp.concatenate([route[...].astype(F32), shares], axis=0)
    bkeys = nq * t_rows
    bspread = (
        lax.broadcasted_iota(jnp.int32, (t_rows, bkeys), 0)
        == (lax.broadcasted_iota(jnp.int32, (t_rows, bkeys), 1) % t_rows)
    ).astype(F32)
    names = jnp.dot(
        names, bspread, preferred_element_type=F32, precision=lax.Precision.HIGHEST
    )
    ri = lax.broadcasted_iota(jnp.int32, (bkeys, bkeys), 0)
    ci = lax.broadcasted_iota(jnp.int32, (bkeys, bkeys), 1)
    tri = ((ri < ci) & ((ri // t_rows) == (ci // t_rows))).astype(F32)
    r = lax.broadcasted_iota(jnp.int32, (n_ep * big, bkeys), 0)
    k = lax.broadcasted_iota(jnp.int32, (n_ep * big, bkeys), 1)
    b = r // big
    s = r % slot
    dz = paired_vec(b // nx, nz)
    dx = paired_vec(b % nx, nx)
    dest = ((my_z + dz) & (nz - 1)) * nx + ((my_x + dx) & (nx - 1))
    slot_e = (dest * n_loc + s // CAP).astype(F32)
    same = ((r // slot) % nq) == (k // t_rows)
    hit0 = (slot_e == names[0:1, :]).astype(F32)
    hit1 = (slot_e == names[1:2, :]).astype(F32)
    before = jnp.dot(hit0 + hit1, tri, preferred_element_type=F32)
    taken = same & (before == (s % CAP).astype(F32))
    combine = jnp.where(taken, hit0 * names[2:3, :] + hit1 * names[3:4, :], 0.0).T
    pr = lax.broadcasted_iota(jnp.int32, (crow, crow), 0)
    pc = lax.broadcasted_iota(jnp.int32, (crow, crow), 1)
    perm = (
        ((pr // xrow) == ((pc // slot) % 2))
        & (((pr // slot) % per) == (pc // blk))
        & ((pr % slot) == (pc % slot))
    ).astype(BF16)
    xr = lax.broadcasted_iota(jnp.int32, (brow, xrow), 0)
    xc = lax.broadcasted_iota(jnp.int32, (brow, xrow), 1)
    expand = (((xr // big) == (xc // slot)) & ((xr % slot) == (xc % slot))).astype(BF16)
    sr = lax.broadcasted_iota(jnp.int32, (brow, 128), 0)
    sc = lax.broadcasted_iota(jnp.int32, (brow, 128), 1)
    in_lane = (sr % big) == sc
    gr = lax.broadcasted_iota(jnp.int32, (per, brow), 0)
    gc = lax.broadcasted_iota(jnp.int32, (per, brow), 1)
    in_block = gr == (gc // big)
    br = lax.broadcasted_iota(jnp.int32, (128, brow), 0)
    bc = lax.broadcasted_iota(jnp.int32, (128, brow), 1)
    unlane = (br == (bc % big)).astype(BF16)
    loads[9].wait()
    for g in range(CORES):
        for q in range(nq):
            for h in range(2):
                at = (CORES * (2 * q + h) + g) * part
                ed[g, q * hid : (q + 1) * hid, h * part : (h + 1) * part] = ednat[
                    :, at : at + part
                ]

    for c in order:
        at = pl.ds(c * per, per - (c == n_chunk - 1))
        remote(
            disp_send.at[at], grid.at[core, row, at], di_s, di_r.at[c], me, tp
        ).wait_recv()
        for d in far_rows:
            spot = grid.at[core, row, chunk(c)]
            remote(spot, spot, ya_s, ya_r.at[c], me, turn(row, d, n_row) * CORES + core).start()

    for i in (3, 4, 5):
        loads[i].wait()
    at = pl.ds(0, n_tp - 1)
    remote(tok.at[at], tok.at[at], ag_s, ag_r, me, tp).wait_recv()
    squares = jnp.zeros((t_rows, part), F32)
    for t in range(n_tp):
        x = tok[t].astype(F32)
        squares += x * x
    inv = lax.rsqrt(jnp.sum(squares, axis=1, keepdims=True) / width + norm_eps)
    mix = jnp.zeros((t_rows, part), F32)
    for t in range(n_tp):
        cols = slice(t * part, (t + 1) * part)
        nt = (tok[t].astype(F32) * inv * gain[:, cols]).astype(BF16)
        normed[:, cols] = nt
        mix += nt.astype(F32) * mixw[:, cols]
    mix_gate = 1.0 / (1.0 + jnp.exp(-jnp.sum(mix, axis=1, keepdims=True)))
    for i in (6, 7, 8):
        loads[i].wait()
    both = lax.dot_general(normed[...], wd[...], NT, preferred_element_type=F32)
    dh = (silu(both[:, 0:ffd]) * both[:, ffd : 2 * ffd]).astype(BF16)
    for t in range(n_tp):
        dense_send[t] = jnp.dot(
            dh, dd[:, t * part : (t + 1) * part], preferred_element_type=F32
        )
    for d in far_tp:
        t = turn(tp, d, n_tp)
        remote(dense_send.at[t], dense_recv.at[d - 1], de_s, de_r, me, t).start()
    for i in (10, 11):
        loads[i].wait()

    def unpack(c, g):
        slabs = [
            grid[g, y, c * per : (c + 1) * per].astype(F32).reshape(crow, half)
            for y in range(n_row)
        ]
        moved = jnp.dot(
            perm, jnp.concatenate(slabs, axis=1).astype(BF16), preferred_element_type=F32
        )
        total = jnp.zeros((xrow, half), F32)
        for y in range(n_row):
            for h in range(2):
                v = moved[h * xrow : (h + 1) * xrow, y * half : (y + 1) * half]
                at = pl.multiple_of((CORES * y + g) * part + h * half, half)
                rows_n[c * xrow : (c + 1) * xrow, pl.ds(at, half)] = v.astype(BF16)
                total += v * v
        return jnp.sum(total, axis=1, keepdims=True)

    ar = lax.broadcasted_iota(jnp.int32, (xrow, hid), 0)
    ac = lax.broadcasted_iota(jnp.int32, (xrow, hid), 1)
    mine = ((ar % slot) // CAP) == (ac // (hid // n_loc))
    hr = lax.broadcasted_iota(jnp.int32, (brow, hid), 0)
    seen = {}

    def gather(c):
        at = pl.ds(0, n_row - 1)
        spot = grid.at[core, at, chunk(c)]
        remote(spot, spot, ya_s, ya_r.at[c], me, tp).wait_recv()
        spot = grid.at[core, :, chunk(c)]
        remote(spot, spot, pf_s, pf_r.at[c], me, partner).start()
        seen[c] = unpack(c, core)

    def apply(c):
        spot = grid.at[1 - core, :, chunk(c)]
        remote(spot, spot, pf_s, pf_r.at[c], me, tp).wait_recv()
        inv = lax.rsqrt((seen[c] + unpack(c, 1 - core)) / width + norm_eps)
        rows = slice(c * xrow, (c + 1) * xrow)
        for t in range(n_tp):
            cols = slice(t * part, (t + 1) * part)
            rows_n[rows, cols] = (rows_n[rows, cols].astype(F32) * inv * gain[:, cols]).astype(
                BF16
            )
        act = lax.dot_general(rows_n[rows, :], wgu[...], NT, preferred_element_type=F32)
        hidden = jnp.where(mine, silu(act[:, 0:hid]) * act[:, hid : 2 * hid], 0.0)
        wider = jnp.dot(expand, hidden.astype(BF16), preferred_element_type=F32)
        rows = slice(c * brow, (c + 1) * brow)
        for q in range(nq):
            hid4[rows, q * hid : (q + 1) * hid] = jnp.where(
                ((hr // slot) % nq) == q, wider, 0.0
            ).astype(BF16)
        pair_send[rows, :] = jnp.dot(hid4[rows, :], ed[1 - core], preferred_element_type=F32)
        at = pl.ds(c * brow, brow)
        remote(pair_send.at[at], pair_recv.at[at], pa_s, pa_r.at[c], me, partner).start()

    def reply(c):
        rows = slice(c * brow, (c + 1) * brow)
        v = jnp.dot(hid4[rows, :], ed[core], preferred_element_type=F32)
        at = pl.ds(c * brow, brow)
        remote(pair_send.at[at], pair_recv.at[at], pa_s, pa_r.at[c], me, tp).wait_recv()
        v = v + pair_recv[rows, :]
        peak = jnp.max(jnp.abs(v), axis=1, keepdims=True)
        step = (jnp.maximum(peak, 1e-30) * (1.0 / 32600.0)).astype(BF16).astype(F32)
        ret_send[rows, :] = (
            jnp.floor(v * (1.0 / step) + 0.5).astype(jnp.int32).astype(jnp.int16)
        )
        lanes = jnp.where(in_lane, step, 0.0).astype(BF16)
        steps = jnp.dot(in_block.astype(BF16), lanes, preferred_element_type=F32)
        for i in range(per):
            j = c * per + i
            scl_send[j] = steps[i : i + 1, :]
            if j < n_ep - 1:
                remote(
                    scl_send.at[j], scl_recv.at[j], sc_s, sc_r.at[c], behind(j), tp
                ).start()
        for i in range(per):
            j = c * per + i
            if j < n_ep - 1:
                at = pl.ds(j * big, big)
                remote(
                    ret_send.at[at], ret_recv.at[at], re_s, re_r.at[c], behind(j), tp
                ).start()
        if c == n_chunk - 1:
            tail = slice((n_ep - 1) * big, n_ep * big)
            ret_recv[tail, :] = ret_send[tail, :]
            scl_recv[n_ep - 1] = scl_send[n_ep - 1]

    for run, i in (
        (gather, 0),
        (apply, 0),
        (gather, 1),
        (reply, 0),
        (apply, 1),
        (gather, 2),
        (reply, 1),
        (gather, 3),
        (apply, 2),
        (apply, 3),
        (reply, 2),
        (reply, 3),
    ):
        run(order[i])
    at = pl.ds(0, n_tp - 1)
    remote(dense_recv.at[at], dense_recv.at[at], de_s, de_r, me, tp).wait_recv()
    total = dense_send[tp]
    for d in range(1, n_tp):
        total += dense_recv[d - 1]
    total = mix_gate * total
    mixed = jnp.zeros((bkeys, wide), F32)
    for c in order:
        n = per - (c == n_chunk - 1)
        at = pl.ds(c * brow, n * big)
        remote(ret_send.at[at], ret_recv.at[at], re_s, re_r.at[c], me, tp).wait_recv()
        at = pl.ds(c * per, n)
        remote(scl_send.at[at], scl_recv.at[at], sc_s, sc_r.at[c], me, tp).wait_recv()
        rows = slice(c * brow, (c + 1) * brow)
        steps = jnp.concatenate([scl_recv[c * per + i] for i in range(per)], axis=0)
        lanes = jnp.dot(steps.astype(BF16), unlane, preferred_element_type=F32)
        step = jnp.sum(jnp.where(in_block, lanes, 0.0), axis=0, keepdims=True)
        back = ret_recv[rows, :].astype(jnp.int32).astype(F32)
        mixed += jnp.dot(
            combine[:, rows] * step,
            back,
            preferred_element_type=F32,
            precision=lax.Precision.HIGHEST,
        )
    for q in range(nq):
        for h in range(2):
            fin_send[2 * q + h] = mixed[
                q * t_rows : (q + 1) * t_rows, h * part : (h + 1) * part
            ]
    for d in far_rows:
        y = turn(row, d, n_row)
        remote(
            fin_send.at[y], fin_recv.at[d - 1], fi_s, fi_r, me, y * CORES + core
        ).start()
    remote(fin_recv, fin_recv, fi_s, fi_r, me, tp).wait_recv()
    total += fin_send[row]
    for d in range(1, n_row):
        total += fin_recv[d - 1]
    eye = lax.broadcasted_iota(jnp.int32, (t_rows, 128), 0) == lax.broadcasted_iota(
        jnp.int32, (t_rows, 128), 1
    )
    mine_sq = jnp.sum(
        jnp.where(eye, jnp.sum(total * total, axis=1, keepdims=True), 0.0),
        axis=0,
        keepdims=True,
    )
    sq_send[...] = mine_sq
    for d in far_tp:
        remote(sq_send, sq_recv.at[d - 1], sq_s, sq_r, me, turn(tp, d, n_tp)).start()
    remote(sq_recv, sq_recv, sq_s, sq_r, me, tp).wait_recv()
    all_sq = mine_sq
    for d in range(1, n_tp):
        all_sq += sq_recv[d - 1]
    all_sq = jnp.sum(jnp.where(eye, all_sq, 0.0), axis=1, keepdims=True)
    scale = lax.rsqrt(all_sq / width + norm_eps)
    out_ref[...] = (total * scale * og[...]).astype(out_ref.dtype)
    at = pl.ds(0, n_tp - 1)
    remote(tok.at[at], tok.at[at], ag_s, ag_r, me, tp).wait_send()
    remote(dense_recv.at[at], dense_recv.at[at], de_s, de_r, me, tp).wait_send()
    remote(sq_recv, sq_recv, sq_s, sq_r, me, tp).wait_send()
    at = pl.ds(0, n_ep - 1)
    remote(disp_send.at[at], disp_send.at[at], di_s, di_r.at[0], me, tp).wait_send()
    remote(scl_send.at[at], scl_recv.at[at], sc_s, sc_r.at[0], me, tp).wait_send()
    at = pl.ds(0, (n_ep - 1) * big)
    remote(ret_send.at[at], ret_recv.at[at], re_s, re_r.at[0], me, tp).wait_send()
    spot = grid.at[0, pl.ds(0, n_row - 1)]
    remote(spot, spot, ya_s, ya_r.at[0], me, tp).wait_send()
    remote(grid.at[0], grid.at[0], pf_s, pf_r.at[0], me, tp).wait_send()
    remote(pair_send, pair_recv, pa_s, pa_r.at[0], me, tp).wait_send()
    remote(fin_recv, fin_recv, fi_s, fi_r, me, tp).wait_send()


def shards(n_ep, n_tp, *args):
    (tok, gain, route, logit, eg, eu, ed, dg, du, dd, mixw, og) = args
    t_rows, part = tok.shape
    width = part * n_tp
    half = part // 2
    n_loc, _, ff = eg.shape
    ffd = dg.shape[1]
    hid = n_loc * ff
    n_row = n_tp // CORES
    slot = n_loc * CAP
    blk = 2 * slot
    nq = n_row // 2
    big = n_ep * nq * slot
    wide = 2 * part
    n_chunk = chunks_of(n_ep)
    dma = pltpu.SemaphoreType.DMA
    V = pltpu.VMEM
    scratch = [
        V((n_tp, t_rows, part), BF16),
        V((1, width), F32),
        V(route.shape[::-1], jnp.int32),
        V(logit.shape[::-1], F32),
        V((2 * hid, width), BF16),
        V((hid, width), BF16),
        V((CORES, nq * hid, wide), BF16),
        V((2 * ffd, width), BF16),
        V(dd.shape, BF16),
        V((1, width), F32),
        V((1, part), F32),
        V((t_rows, width), BF16),
        V((n_ep, blk, half), BF16),
        V((CORES, n_row, n_ep, blk, half), BF16),
        V((n_ep * slot, width), BF16),
        V((big, nq * hid), BF16),
        V((n_tp, t_rows, part), F32),
        V((n_tp - 1, t_rows, part), F32),
        V((big, wide), F32),
        V((big, wide), F32),
        V((big, wide), jnp.int16),
        V((big, wide), jnp.int16),
        V((n_ep, 1, 128), F32),
        V((n_ep, 1, 128), F32),
        V((n_row, t_rows, part), F32),
        V((n_row - 1, t_rows, part), F32),
        V((1, 128), F32),
        V((n_tp - 1, 1, 128), F32),
        dma((12,)),
        dma,
        dma,
        dma,
        dma((n_chunk,)),
        dma,
        dma((n_chunk,)),
        dma,
        dma((n_chunk,)),
        dma,
        dma,
        dma,
        dma((n_chunk,)),
        dma,
        dma((n_chunk,)),
        dma,
        dma((n_chunk,)),
        dma,
        dma,
        dma,
        dma,
    ]
    return pl.pallas_call(
        functools.partial(kernel, n_ep, n_tp, n_loc),
        out_shape=jax.ShapeDtypeStruct((t_rows, part), BF16),
        in_specs=[pl.BlockSpec(memory_space=pltpu.HBM)] * 12,
        out_specs=pl.BlockSpec(memory_space=pltpu.VMEM),
        scratch_shapes=scratch,
        compiler_params=pltpu.CompilerParams(
            collective_id=0, has_side_effects=True, vmem_limit_bytes=60 * 1024 * 1024
        ),
        name="moe_layer",
    )(
        tok,
        gain.reshape(1, width),
        route.T,
        logit.T,
        eg.swapaxes(1, 2).reshape(hid, width),
        eu.swapaxes(1, 2).reshape(hid, width),
        ed.reshape(hid, width),
        dg.T,
        du.T,
        dd,
        mixw.reshape(1, width),
        og.reshape(1, part),
    )


def solution(mesh):
    placed = (
        P("ep", "tp"),
        P(),
        P("ep", None),
        P("ep", None),
        P("ep", None, "tp"),
        P("ep", None, "tp"),
        P("ep", "tp", None),
        P(None, "tp"),
        P(None, "tp"),
        P("tp", None),
        P(),
        P("tp"),
    )
    return jax.shard_map(
        functools.partial(shards, mesh.shape["ep"], mesh.shape["tp"]),
        mesh=mesh,
        in_specs=placed,
        out_specs=P("ep", "tp"),
        check_vma=False,
    )
```

```python
import functools

import jax
import jax.numpy as jnp
from jax import lax
from jax.experimental import pallas as pl
from jax.experimental.pallas import tpu as pltpu
from jax.sharding import PartitionSpec as P

CAP = 2
CORES = 2
NX = 4
CHUNKS = 4
norm_eps = 1e-06
MESH = pl.DeviceIdType.MESH
F32 = jnp.float32
BF16 = jnp.bfloat16
NT = (((1,), (1,)), ((), ()))


def silu(v):
    return v / (1.0 + jnp.exp(-v))


def chunks_of(n_ep):
    return CHUNKS if n_ep >= 2 * CHUNKS else 2


def paired(i, n):
    h = n // 2 - 1 - i // 2
    if i < n - 2:
        return h if i % 2 == 0 else n - h
    return n // 2 if i == n - 2 else 0


def paired_vec(i, n):
    h = n // 2 - 1 - (i >> 1)
    return jnp.where(
        i < n - 2,
        jnp.where((i & 1) == 0, h, n - h),
        jnp.where(i == n - 2, n // 2, 0),
    )


def kernel(
    n_ep,
    n_tp,
    n_loc,
    tok_hbm,
    gain_hbm,
    route_hbm,
    logit_hbm,
    eg_hbm,
    eu_hbm,
    ed_hbm,
    dg_hbm,
    du_hbm,
    dd_hbm,
    mix_hbm,
    og_hbm,
    out_ref,
    tok,
    gain,
    route,
    logit,
    wgu,
    ednat,
    ed,
    wd,
    dd,
    mixw,
    og,
    normed,
    disp_send,
    grid,
    rows_n,
    hid4,
    dense_send,
    dense_recv,
    pair_send,
    pair_recv,
    ret_send,
    ret_recv,
    scl_send,
    scl_recv,
    fin_send,
    fin_recv,
    sq_send,
    sq_recv,
    lsem,
    ag_s,
    ag_r,
    di_s,
    di_r,
    ya_s,
    ya_r,
    pf_s,
    pf_r,
    de_s,
    de_r,
    pa_s,
    pa_r,
    re_s,
    re_r,
    sc_s,
    sc_r,
    fi_s,
    fi_r,
    sq_s,
    sq_r,
):
    me = lax.axis_index("ep")
    tp = lax.axis_index("tp")
    core = lax.rem(tp, CORES)
    row = lax.div(tp, CORES)
    n_row = n_tp // CORES
    partner = row * CORES + (1 - core)
    t_rows, part = tok.shape[1], tok.shape[2]
    width = part * n_tp
    half = part // 2
    nx = min(NX, n_ep)
    nz = n_ep // nx
    both_ways = min(2, nz)
    my_z = lax.div(me, nx)
    my_x = lax.rem(me, nx)
    slot = n_loc * CAP
    blk = 2 * slot
    slots = n_ep * blk
    keys = 2 * t_rows
    hid = ednat.shape[0]
    n_chunk = chunks_of(n_ep)
    order = [0, 3, 1, 2]
    per = n_ep // n_chunk
    crow = per * blk
    xrow = per * slot
    nq = n_row // 2
    big = nq * slot
    brow = per * big
    wide = 2 * part
    far_rows = sorted(range(1, n_row), key=lambda d: -min(d, n_row - d))
    far_tp = sorted(range(1, n_tp), key=lambda d: -min(d, n_tp - d))

    def turn(base, d, n):
        return lax.rem(base + d, n)

    def remote(src, dst, s, r, e, t):
        return pltpu.make_async_remote_copy(
            src_ref=src,
            dst_ref=dst,
            send_sem=s,
            recv_sem=r,
            device_id={"ep": e, "tp": t},
            device_id_type=MESH,
        )

    def offsets(b):
        iz = both_ways * (b // (both_ways * nx)) + b % both_ways
        return paired(iz, nz), paired(b % (both_ways * nx) // both_ways, nx)

    def ahead(b):
        dz, dx = offsets(b)
        return turn(my_z, dz, nz) * nx + turn(my_x, dx, nx)

    def behind(b):
        dz, dx = offsets(b)
        return turn(my_z, (nz - dz) % nz, nz) * nx + turn(my_x, (nx - dx) % nx, nx)

    def chunk(c):
        return pl.ds(c * per, per)

    half_w = wgu.shape[0] // 2
    ffd = wd.shape[0] // 2
    loads = []
    pairs = [
        (tok_hbm, tok.at[tp]),
        (route_hbm, route),
        (logit_hbm, logit),
        (gain_hbm, gain),
        (mix_hbm, mixw),
        (og_hbm, og),
        (dg_hbm, wd.at[0:ffd]),
        (du_hbm, wd.at[ffd : 2 * ffd]),
        (dd_hbm, dd),
        (ed_hbm, ednat),
        (eg_hbm, wgu.at[0:half_w]),
        (eu_hbm, wgu.at[half_w : 2 * half_w]),
    ]
    for i, (src, dst) in enumerate(pairs):
        loads.append(pltpu.make_async_copy(src, dst, lsem.at[i]))
    for c in loads[0:2]:
        c.start()
    barrier = pltpu.get_barrier_semaphore()
    greeted = 0
    for j in range(n_ep - 1):
        pl.semaphore_signal(
            barrier, inc=1, device_id={"ep": ahead(j), "tp": tp}, device_id_type=MESH
        )
        greeted += 1
    for d in far_tp:
        pl.semaphore_signal(
            barrier, inc=1, device_id={"ep": me, "tp": turn(tp, d, n_tp)}, device_id_type=MESH
        )
        greeted += 1
    for c in loads[2:]:
        c.start()

    loads[1].wait()
    spread = (
        lax.broadcasted_iota(jnp.int32, (t_rows, keys), 0)
        == (lax.broadcasted_iota(jnp.int32, (t_rows, keys), 1) % t_rows)
    ).astype(F32)
    both = jnp.dot(route[...].astype(F32), spread, preferred_element_type=F32)
    ri = lax.broadcasted_iota(jnp.int32, (keys, keys), 0)
    ci = lax.broadcasted_iota(jnp.int32, (keys, keys), 1)
    tri = ((ri < ci) & ((ri // t_rows) == (ci // t_rows))).astype(F32)
    r = lax.broadcasted_iota(jnp.int32, (slots, keys), 0)
    k = lax.broadcasted_iota(jnp.int32, (slots, keys), 1)
    b = r // blk
    s = r % slot
    dz = paired_vec(both_ways * (b // (both_ways * nx)) + b % both_ways, nz)
    dx = paired_vec((b % (both_ways * nx)) // both_ways, nx)
    dest = ((my_z + dz) & (nz - 1)) * nx + ((my_x + dx) & (nx - 1))
    slot_e = (dest * n_loc + s // CAP).astype(F32)
    same = ((r // slot) % 2) == (k // t_rows)
    hit0 = (slot_e == both[0:1, :]).astype(F32)
    hit1 = (slot_e == both[1:2, :]).astype(F32)
    hits = hit0 + hit1
    before = jnp.dot(hits, tri, preferred_element_type=F32)
    place = jnp.where(same & (before == (s % CAP).astype(F32)), hits, 0.0)
    loads[0].wait()
    x = tok[tp].astype(F32)
    source = jnp.concatenate([x[:, 0:half], x[:, half:part]], axis=0).astype(BF16)
    placed = jnp.dot(place.astype(BF16), source, preferred_element_type=F32)
    placed = placed.reshape(n_ep, blk, half).astype(BF16)
    disp_send[...] = placed
    pl.semaphore_wait(barrier, greeted)
    for j in range(n_ep - 1):
        remote(
            disp_send.at[j], grid.at[core, row, j], di_s, di_r.at[j // per], ahead(j), tp
        ).start()
    for d in far_tp:
        remote(tok.at[tp], tok.at[tp], ag_s, ag_r, me, turn(tp, d, n_tp)).start()
    grid[core, row, n_ep - 1] = placed[n_ep - 1]

    loads[2].wait()
    l0 = logit[0:1, :]
    l1 = logit[1:2, :]
    top = jnp.maximum(l0, l1)
    e0 = jnp.exp(l0 - top)
    e1 = jnp.exp(l1 - top)
    shares = jnp.concatenate([e0 / (e0 + e1), e1 / (e0 + e1)], axis=0)
    names = jnp.concatenate([route[...].astype(F32), shares], axis=0)
    bkeys = nq * t_rows
    bspread = (
        lax.broadcasted_iota(jnp.int32, (t_rows, bkeys), 0)
        == (lax.broadcasted_iota(jnp.int32, (t_rows, bkeys), 1) % t_rows)
    ).astype(F32)
    names = jnp.dot(
        names, bspread, preferred_element_type=F32, precision=lax.Precision.HIGHEST
    )
    ri = lax.broadcasted_iota(jnp.int32, (bkeys, bkeys), 0)
    ci = lax.broadcasted_iota(jnp.int32, (bkeys, bkeys), 1)
    tri = ((ri < ci) & ((ri // t_rows) == (ci // t_rows))).astype(F32)
    r = lax.broadcasted_iota(jnp.int32, (n_ep * big, bkeys), 0)
    k = lax.broadcasted_iota(jnp.int32, (n_ep * big, bkeys), 1)
    b = r // big
    s = r % slot
    dz = paired_vec(both_ways * (b // (both_ways * nx)) + b % both_ways, nz)
    dx = paired_vec((b % (both_ways * nx)) // both_ways, nx)
    dest = ((my_z + dz) & (nz - 1)) * nx + ((my_x + dx) & (nx - 1))
    slot_e = (dest * n_loc + s // CAP).astype(F32)
    same = ((r // slot) % nq) == (k // t_rows)
    hit0 = (slot_e == names[0:1, :]).astype(F32)
    hit1 = (slot_e == names[1:2, :]).astype(F32)
    before = jnp.dot(hit0 + hit1, tri, preferred_element_type=F32)
    taken = same & (before == (s % CAP).astype(F32))
    combine = jnp.where(taken, hit0 * names[2:3, :] + hit1 * names[3:4, :], 0.0).T
    pr = lax.broadcasted_iota(jnp.int32, (crow, crow), 0)
    pc = lax.broadcasted_iota(jnp.int32, (crow, crow), 1)
    perm = (
        ((pr // xrow) == ((pc // slot) % 2))
        & (((pr // slot) % per) == (pc // blk))
        & ((pr % slot) == (pc % slot))
    ).astype(BF16)
    xr = lax.broadcasted_iota(jnp.int32, (brow, xrow), 0)
    xc = lax.broadcasted_iota(jnp.int32, (brow, xrow), 1)
    expand = (((xr // big) == (xc // slot)) & ((xr % slot) == (xc % slot))).astype(BF16)
    sr = lax.broadcasted_iota(jnp.int32, (brow, 128), 0)
    sc = lax.broadcasted_iota(jnp.int32, (brow, 128), 1)
    in_lane = (sr % big) == sc
    gr = lax.broadcasted_iota(jnp.int32, (per, brow), 0)
    gc = lax.broadcasted_iota(jnp.int32, (per, brow), 1)
    in_block = gr == (gc // big)
    br = lax.broadcasted_iota(jnp.int32, (128, brow), 0)
    bc = lax.broadcasted_iota(jnp.int32, (128, brow), 1)
    unlane = (br == (bc % big)).astype(BF16)
    loads[9].wait()
    for g in range(CORES):
        for q in range(nq):
            for h in range(2):
                at = (CORES * (2 * q + h) + g) * part
                ed[g, q * hid : (q + 1) * hid, h * part : (h + 1) * part] = ednat[
                    :, at : at + part
                ]

    for c in order:
        at = pl.ds(c * per, per - (c == n_chunk - 1))
        remote(
            disp_send.at[at], grid.at[core, row, at], di_s, di_r.at[c], me, tp
        ).wait_recv()
        for d in far_rows:
            spot = grid.at[core, row, chunk(c)]
            remote(spot, spot, ya_s, ya_r.at[c], me, turn(row, d, n_row) * CORES + core).start()

    for i in (3, 4, 5):
        loads[i].wait()
    at = pl.ds(0, n_tp - 1)
    remote(tok.at[at], tok.at[at], ag_s, ag_r, me, tp).wait_recv()
    squares = jnp.zeros((t_rows, part), F32)
    for t in range(n_tp):
        x = tok[t].astype(F32)
        squares += x * x
    inv = lax.rsqrt(jnp.sum(squares, axis=1, keepdims=True) / width + norm_eps)
    mix = jnp.zeros((t_rows, part), F32)
    for t in range(n_tp):
        cols = slice(t * part, (t + 1) * part)
        nt = (tok[t].astype(F32) * inv * gain[:, cols]).astype(BF16)
        normed[:, cols] = nt
        mix += nt.astype(F32) * mixw[:, cols]
    mix_gate = 1.0 / (1.0 + jnp.exp(-jnp.sum(mix, axis=1, keepdims=True)))
    for i in (6, 7, 8):
        loads[i].wait()
    both = lax.dot_general(normed[...], wd[...], NT, preferred_element_type=F32)
    dh = (silu(both[:, 0:ffd]) * both[:, ffd : 2 * ffd]).astype(BF16)
    for t in range(n_tp):
        dense_send[t] = jnp.dot(
            dh, dd[:, t * part : (t + 1) * part], preferred_element_type=F32
        )
    for d in far_tp:
        t = turn(tp, d, n_tp)
        remote(dense_send.at[t], dense_recv.at[d - 1], de_s, de_r, me, t).start()
    for i in (10, 11):
        loads[i].wait()

    def unpack(c, g):
        slabs = [
            grid[g, y, c * per : (c + 1) * per].astype(F32).reshape(crow, half)
            for y in range(n_row)
        ]
        moved = jnp.dot(
            perm, jnp.concatenate(slabs, axis=1).astype(BF16), preferred_element_type=F32
        )
        total = jnp.zeros((xrow, half), F32)
        for y in range(n_row):
            for h in range(2):
                v = moved[h * xrow : (h + 1) * xrow, y * half : (y + 1) * half]
                at = pl.multiple_of((CORES * y + g) * part + h * half, half)
                rows_n[c * xrow : (c + 1) * xrow, pl.ds(at, half)] = v.astype(BF16)
                total += v * v
        return jnp.sum(total, axis=1, keepdims=True)

    ar = lax.broadcasted_iota(jnp.int32, (xrow, hid), 0)
    ac = lax.broadcasted_iota(jnp.int32, (xrow, hid), 1)
    mine = ((ar % slot) // CAP) == (ac // (hid // n_loc))
    hr = lax.broadcasted_iota(jnp.int32, (brow, hid), 0)
    seen = {}

    def gather(c):
        at = pl.ds(0, n_row - 1)
        spot = grid.at[core, at, chunk(c)]
        remote(spot, spot, ya_s, ya_r.at[c], me, tp).wait_recv()
        spot = grid.at[core, :, chunk(c)]
        remote(spot, spot, pf_s, pf_r.at[c], me, partner).start()
        seen[c] = unpack(c, core)

    def apply(c):
        spot = grid.at[1 - core, :, chunk(c)]
        remote(spot, spot, pf_s, pf_r.at[c], me, tp).wait_recv()
        inv = lax.rsqrt((seen[c] + unpack(c, 1 - core)) / width + norm_eps)
        rows = slice(c * xrow, (c + 1) * xrow)
        for t in range(n_tp):
            cols = slice(t * part, (t + 1) * part)
            rows_n[rows, cols] = (rows_n[rows, cols].astype(F32) * inv * gain[:, cols]).astype(
                BF16
            )
        act = lax.dot_general(rows_n[rows, :], wgu[...], NT, preferred_element_type=F32)
        hidden = jnp.where(mine, silu(act[:, 0:hid]) * act[:, hid : 2 * hid], 0.0)
        wider = jnp.dot(expand, hidden.astype(BF16), preferred_element_type=F32)
        rows = slice(c * brow, (c + 1) * brow)
        for q in range(nq):
            hid4[rows, q * hid : (q + 1) * hid] = jnp.where(
                ((hr // slot) % nq) == q, wider, 0.0
            ).astype(BF16)
        pair_send[rows, :] = jnp.dot(hid4[rows, :], ed[1 - core], preferred_element_type=F32)
        at = pl.ds(c * brow, brow)
        remote(pair_send.at[at], pair_recv.at[at], pa_s, pa_r.at[c], me, partner).start()

    def reply(c):
        rows = slice(c * brow, (c + 1) * brow)
        v = jnp.dot(hid4[rows, :], ed[core], preferred_element_type=F32)
        at = pl.ds(c * brow, brow)
        remote(pair_send.at[at], pair_recv.at[at], pa_s, pa_r.at[c], me, tp).wait_recv()
        v = v + pair_recv[rows, :]
        peak = jnp.max(jnp.abs(v), axis=1, keepdims=True)
        step = (jnp.maximum(peak, 1e-30) * (1.0 / 32600.0)).astype(BF16).astype(F32)
        ret_send[rows, :] = (
            jnp.floor(v * (1.0 / step) + 0.5).astype(jnp.int32).astype(jnp.int16)
        )
        lanes = jnp.where(in_lane, step, 0.0).astype(BF16)
        steps = jnp.dot(in_block.astype(BF16), lanes, preferred_element_type=F32)
        for i in range(per):
            j = c * per + i
            scl_send[j] = steps[i : i + 1, :]
            if j < n_ep - 1:
                remote(
                    scl_send.at[j], scl_recv.at[j], sc_s, sc_r.at[c], behind(j), tp
                ).start()
        for i in range(per):
            j = c * per + i
            if j < n_ep - 1:
                at = pl.ds(j * big, big)
                remote(
                    ret_send.at[at], ret_recv.at[at], re_s, re_r.at[c], behind(j), tp
                ).start()
        if c == n_chunk - 1:
            tail = slice((n_ep - 1) * big, n_ep * big)
            ret_recv[tail, :] = ret_send[tail, :]
            scl_recv[n_ep - 1] = scl_send[n_ep - 1]

    for run, i in (
        (gather, 0),
        (apply, 0),
        (gather, 1),
        (reply, 0),
        (apply, 1),
        (gather, 2),
        (reply, 1),
        (gather, 3),
        (apply, 2),
        (apply, 3),
        (reply, 2),
        (reply, 3),
    ):
        run(order[i])
    at = pl.ds(0, n_tp - 1)
    remote(dense_recv.at[at], dense_recv.at[at], de_s, de_r, me, tp).wait_recv()
    total = dense_send[tp]
    for d in range(1, n_tp):
        total += dense_recv[d - 1]
    total = mix_gate * total
    mixed = jnp.zeros((bkeys, wide), F32)
    for c in order:
        n = per - (c == n_chunk - 1)
        at = pl.ds(c * brow, n * big)
        remote(ret_send.at[at], ret_recv.at[at], re_s, re_r.at[c], me, tp).wait_recv()
        at = pl.ds(c * per, n)
        remote(scl_send.at[at], scl_recv.at[at], sc_s, sc_r.at[c], me, tp).wait_recv()
        rows = slice(c * brow, (c + 1) * brow)
        steps = jnp.concatenate([scl_recv[c * per + i] for i in range(per)], axis=0)
        lanes = jnp.dot(steps.astype(BF16), unlane, preferred_element_type=F32)
        step = jnp.sum(jnp.where(in_block, lanes, 0.0), axis=0, keepdims=True)
        back = ret_recv[rows, :].astype(jnp.int32).astype(F32)
        mixed += jnp.dot(
            combine[:, rows] * step,
            back,
            preferred_element_type=F32,
            precision=lax.Precision.HIGHEST,
        )
    for q in range(nq):
        for h in range(2):
            fin_send[2 * q + h] = mixed[
                q * t_rows : (q + 1) * t_rows, h * part : (h + 1) * part
            ]
    for d in far_rows:
        y = turn(row, d, n_row)
        remote(
            fin_send.at[y], fin_recv.at[d - 1], fi_s, fi_r, me, y * CORES + core
        ).start()
    remote(fin_recv, fin_recv, fi_s, fi_r, me, tp).wait_recv()
    total += fin_send[row]
    for d in range(1, n_row):
        total += fin_recv[d - 1]
    eye = lax.broadcasted_iota(jnp.int32, (t_rows, 128), 0) == lax.broadcasted_iota(
        jnp.int32, (t_rows, 128), 1
    )
    mine_sq = jnp.sum(
        jnp.where(eye, jnp.sum(total * total, axis=1, keepdims=True), 0.0),
        axis=0,
        keepdims=True,
    )
    sq_send[...] = mine_sq
    for d in far_tp:
        remote(sq_send, sq_recv.at[d - 1], sq_s, sq_r, me, turn(tp, d, n_tp)).start()
    remote(sq_recv, sq_recv, sq_s, sq_r, me, tp).wait_recv()
    all_sq = mine_sq
    for d in range(1, n_tp):
        all_sq += sq_recv[d - 1]
    all_sq = jnp.sum(jnp.where(eye, all_sq, 0.0), axis=1, keepdims=True)
    scale = lax.rsqrt(all_sq / width + norm_eps)
    out_ref[...] = (total * scale * og[...]).astype(out_ref.dtype)
    at = pl.ds(0, n_tp - 1)
    remote(tok.at[at], tok.at[at], ag_s, ag_r, me, tp).wait_send()
    remote(dense_recv.at[at], dense_recv.at[at], de_s, de_r, me, tp).wait_send()
    remote(sq_recv, sq_recv, sq_s, sq_r, me, tp).wait_send()
    at = pl.ds(0, n_ep - 1)
    remote(disp_send.at[at], disp_send.at[at], di_s, di_r.at[0], me, tp).wait_send()
    remote(scl_send.at[at], scl_recv.at[at], sc_s, sc_r.at[0], me, tp).wait_send()
    at = pl.ds(0, (n_ep - 1) * big)
    remote(ret_send.at[at], ret_recv.at[at], re_s, re_r.at[0], me, tp).wait_send()
    spot = grid.at[0, pl.ds(0, n_row - 1)]
    remote(spot, spot, ya_s, ya_r.at[0], me, tp).wait_send()
    remote(grid.at[0], grid.at[0], pf_s, pf_r.at[0], me, tp).wait_send()
    remote(pair_send, pair_recv, pa_s, pa_r.at[0], me, tp).wait_send()
    remote(fin_recv, fin_recv, fi_s, fi_r, me, tp).wait_send()


def shards(n_ep, n_tp, *args):
    (tok, gain, route, logit, eg, eu, ed, dg, du, dd, mixw, og) = args
    t_rows, part = tok.shape
    width = part * n_tp
    half = part // 2
    n_loc, _, ff = eg.shape
    ffd = dg.shape[1]
    hid = n_loc * ff
    n_row = n_tp // CORES
    slot = n_loc * CAP
    blk = 2 * slot
    nq = n_row // 2
    big = n_ep * nq * slot
    wide = 2 * part
    n_chunk = chunks_of(n_ep)
    dma = pltpu.SemaphoreType.DMA
    V = pltpu.VMEM
    scratch = [
        V((n_tp, t_rows, part), BF16),
        V((1, width), F32),
        V(route.shape[::-1], jnp.int32),
        V(logit.shape[::-1], F32),
        V((2 * hid, width), BF16),
        V((hid, width), BF16),
        V((CORES, nq * hid, wide), BF16),
        V((2 * ffd, width), BF16),
        V(dd.shape, BF16),
        V((1, width), F32),
        V((1, part), F32),
        V((t_rows, width), BF16),
        V((n_ep, blk, half), BF16),
        V((CORES, n_row, n_ep, blk, half), BF16),
        V((n_ep * slot, width), BF16),
        V((big, nq * hid), BF16),
        V((n_tp, t_rows, part), F32),
        V((n_tp - 1, t_rows, part), F32),
        V((big, wide), F32),
        V((big, wide), F32),
        V((big, wide), jnp.int16),
        V((big, wide), jnp.int16),
        V((n_ep, 1, 128), F32),
        V((n_ep, 1, 128), F32),
        V((n_row, t_rows, part), F32),
        V((n_row - 1, t_rows, part), F32),
        V((1, 128), F32),
        V((n_tp - 1, 1, 128), F32),
        dma((12,)),
        dma,
        dma,
        dma,
        dma((n_chunk,)),
        dma,
        dma((n_chunk,)),
        dma,
        dma((n_chunk,)),
        dma,
        dma,
        dma,
        dma((n_chunk,)),
        dma,
        dma((n_chunk,)),
        dma,
        dma((n_chunk,)),
        dma,
        dma,
        dma,
        dma,
    ]
    return pl.pallas_call(
        functools.partial(kernel, n_ep, n_tp, n_loc),
        out_shape=jax.ShapeDtypeStruct((t_rows, part), BF16),
        in_specs=[pl.BlockSpec(memory_space=pltpu.HBM)] * 12,
        out_specs=pl.BlockSpec(memory_space=pltpu.VMEM),
        scratch_shapes=scratch,
        compiler_params=pltpu.CompilerParams(
            collective_id=0, has_side_effects=True, vmem_limit_bytes=60 * 1024 * 1024
        ),
        name="moe_layer",
    )(
        tok,
        gain.reshape(1, width),
        route.T,
        logit.T,
        eg.swapaxes(1, 2).reshape(hid, width),
        eu.swapaxes(1, 2).reshape(hid, width),
        ed.reshape(hid, width),
        dg.T,
        du.T,
        dd,
        mixw.reshape(1, width),
        og.reshape(1, part),
    )


def solution(mesh):
    placed = (
        P("ep", "tp"),
        P(),
        P("ep", None),
        P("ep", None),
        P("ep", None, "tp"),
        P("ep", None, "tp"),
        P("ep", "tp", None),
        P(None, "tp"),
        P(None, "tp"),
        P("tp", None),
        P(),
        P("tp"),
    )
    return jax.shard_map(
        functools.partial(shards, mesh.shape["ep"], mesh.shape["tp"]),
        mesh=mesh,
        in_specs=placed,
        out_specs=P("ep", "tp"),
        check_vma=False,
    )
```

```python
import functools

import jax
import jax.numpy as jnp
from jax import lax
from jax.experimental import pallas as pl
from jax.experimental.pallas import tpu as pltpu
from jax.sharding import PartitionSpec as P

CAP = 2
CORES = 2
NX = 4
CHUNKS = 4
norm_eps = 1e-06
MESH = pl.DeviceIdType.MESH
F32 = jnp.float32
BF16 = jnp.bfloat16
NT = (((1,), (1,)), ((), ()))


def silu(v):
    return v / (1.0 + jnp.exp(-v))


def chunks_of(n_ep):
    return CHUNKS if n_ep >= 2 * CHUNKS else 2


def paired(i, n):
    h = n // 2 - 1 - i // 2
    if i < n - 2:
        return h if i % 2 == 0 else n - h
    return n // 2 if i == n - 2 else 0


def paired_vec(i, n):
    h = n // 2 - 1 - (i >> 1)
    return jnp.where(
        i < n - 2,
        jnp.where((i & 1) == 0, h, n - h),
        jnp.where(i == n - 2, n // 2, 0),
    )


def kernel(
    n_ep,
    n_tp,
    n_loc,
    tok_hbm,
    gain_hbm,
    route_hbm,
    logit_hbm,
    eg_hbm,
    eu_hbm,
    ed_hbm,
    dg_hbm,
    du_hbm,
    dd_hbm,
    mix_hbm,
    og_hbm,
    out_ref,
    tok,
    gain,
    route,
    logit,
    wgu,
    ednat,
    ed,
    wd,
    dd,
    mixw,
    og,
    normed,
    disp_send,
    grid,
    rows_n,
    hid4,
    dense_send,
    dense_recv,
    pair_send,
    pair_recv,
    ret_send,
    ret_recv,
    scl_send,
    scl_recv,
    fin_send,
    fin_recv,
    sq_send,
    sq_recv,
    lsem,
    ag_s,
    ag_r,
    di_s,
    di_r,
    ya_s,
    ya_r,
    pf_s,
    pf_r,
    de_s,
    de_r,
    pa_s,
    pa_r,
    re_s,
    re_r,
    sc_s,
    sc_r,
    fi_s,
    fi_r,
    sq_s,
    sq_r,
):
    me = lax.axis_index("ep")
    tp = lax.axis_index("tp")
    core = lax.rem(tp, CORES)
    row = lax.div(tp, CORES)
    n_row = n_tp // CORES
    partner = row * CORES + (1 - core)
    t_rows, part = tok.shape[1], tok.shape[2]
    width = part * n_tp
    half = part // 2
    nx = min(NX, n_ep)
    nz = n_ep // nx
    both_ways = min(2, nz)
    my_z = lax.div(me, nx)
    my_x = lax.rem(me, nx)
    slot = n_loc * CAP
    blk = 2 * slot
    slots = n_ep * blk
    keys = 2 * t_rows
    hid = ednat.shape[0]
    n_chunk = chunks_of(n_ep)
    order = [0, 3, 1, 2]
    per = n_ep // n_chunk
    crow = per * blk
    xrow = per * slot
    nq = n_row // 2
    big = nq * slot
    brow = per * big
    wide = 2 * part
    far_rows = sorted(range(1, n_row), key=lambda d: -min(d, n_row - d))
    far_tp = sorted(range(1, n_tp), key=lambda d: -min(d, n_tp - d))

    def turn(base, d, n):
        return lax.rem(base + d, n)

    def remote(src, dst, s, r, e, t):
        return pltpu.make_async_remote_copy(
            src_ref=src,
            dst_ref=dst,
            send_sem=s,
            recv_sem=r,
            device_id={"ep": e, "tp": t},
            device_id_type=MESH,
        )

    def offsets(b):
        iz = both_ways * (b // (both_ways * nx)) + b % both_ways
        return paired(iz, nz), paired(b % (both_ways * nx) // both_ways, nx)

    def ahead(b):
        dz, dx = offsets(b)
        return turn(my_z, dz, nz) * nx + turn(my_x, dx, nx)

    def behind(b):
        dz, dx = offsets(b)
        return turn(my_z, (nz - dz) % nz, nz) * nx + turn(my_x, (nx - dx) % nx, nx)

    def chunk(c):
        return pl.ds(c * per, per)

    half_w = wgu.shape[0] // 2
    ffd = wd.shape[0] // 2
    loads = []
    pairs = [
        (tok_hbm, tok.at[tp]),
        (route_hbm, route),
        (logit_hbm, logit),
        (gain_hbm, gain),
        (mix_hbm, mixw),
        (og_hbm, og),
        (dg_hbm, wd.at[0:ffd]),
        (du_hbm, wd.at[ffd : 2 * ffd]),
        (dd_hbm, dd),
        (ed_hbm, ednat),
        (eg_hbm, wgu.at[0:half_w]),
        (eu_hbm, wgu.at[half_w : 2 * half_w]),
    ]
    for i, (src, dst) in enumerate(pairs):
        loads.append(pltpu.make_async_copy(src, dst, lsem.at[i]))
    for c in loads[0:2]:
        c.start()
    barrier = pltpu.get_barrier_semaphore()
    greeted = 0
    for j in range(n_ep - 1):
        pl.semaphore_signal(
            barrier, inc=1, device_id={"ep": ahead(j), "tp": tp}, device_id_type=MESH
        )
        greeted += 1
    for d in far_tp:
        pl.semaphore_signal(
            barrier, inc=1, device_id={"ep": me, "tp": turn(tp, d, n_tp)}, device_id_type=MESH
        )
        greeted += 1
    for c in loads[2:]:
        c.start()

    loads[1].wait()
    spread = (
        lax.broadcasted_iota(jnp.int32, (t_rows, keys), 0)
        == (lax.broadcasted_iota(jnp.int32, (t_rows, keys), 1) % t_rows)
    ).astype(F32)
    both = jnp.dot(route[...].astype(F32), spread, preferred_element_type=F32)
    ri = lax.broadcasted_iota(jnp.int32, (keys, keys), 0)
    ci = lax.broadcasted_iota(jnp.int32, (keys, keys), 1)
    tri = ((ri < ci) & ((ri // t_rows) == (ci // t_rows))).astype(F32)
    r = lax.broadcasted_iota(jnp.int32, (slots, keys), 0)
    k = lax.broadcasted_iota(jnp.int32, (slots, keys), 1)
    b = r // blk
    s = r % slot
    dz = paired_vec(both_ways * (b // (both_ways * nx)) + b % both_ways, nz)
    dx = paired_vec((b % (both_ways * nx)) // both_ways, nx)
    dest = ((my_z + dz) & (nz - 1)) * nx + ((my_x + dx) & (nx - 1))
    slot_e = (dest * n_loc + s // CAP).astype(F32)
    same = ((r // slot) % 2) == (k // t_rows)
    hit0 = (slot_e == both[0:1, :]).astype(F32)
    hit1 = (slot_e == both[1:2, :]).astype(F32)
    hits = hit0 + hit1
    before = jnp.dot(hits, tri, preferred_element_type=F32)
    place = jnp.where(same & (before == (s % CAP).astype(F32)), hits, 0.0)
    loads[0].wait()
    x = tok[tp].astype(F32)
    source = jnp.concatenate([x[:, 0:half], x[:, half:part]], axis=0).astype(BF16)
    placed = jnp.dot(place.astype(BF16), source, preferred_element_type=F32)
    placed = placed.reshape(n_ep, blk, half).astype(BF16)
    disp_send[...] = placed
    pl.semaphore_wait(barrier, greeted)
    for j in range(n_ep - 1):
        remote(
            disp_send.at[j], grid.at[core, row, j], di_s, di_r.at[j // per], ahead(j), tp
        ).start()
    for d in far_tp:
        remote(tok.at[tp], tok.at[tp], ag_s, ag_r, me, turn(tp, d, n_tp)).start()
    grid[core, row, n_ep - 1] = placed[n_ep - 1]

    loads[2].wait()
    l0 = logit[0:1, :]
    l1 = logit[1:2, :]
    top = jnp.maximum(l0, l1)
    e0 = jnp.exp(l0 - top)
    e1 = jnp.exp(l1 - top)
    shares = jnp.concatenate([e0 / (e0 + e1), e1 / (e0 + e1)], axis=0)
    names = jnp.concatenate([route[...].astype(F32), shares], axis=0)
    bkeys = nq * t_rows
    bspread = (
        lax.broadcasted_iota(jnp.int32, (t_rows, bkeys), 0)
        == (lax.broadcasted_iota(jnp.int32, (t_rows, bkeys), 1) % t_rows)
    ).astype(F32)
    names = jnp.dot(
        names, bspread, preferred_element_type=F32, precision=lax.Precision.HIGHEST
    )
    ri = lax.broadcasted_iota(jnp.int32, (bkeys, bkeys), 0)
    ci = lax.broadcasted_iota(jnp.int32, (bkeys, bkeys), 1)
    tri = ((ri < ci) & ((ri // t_rows) == (ci // t_rows))).astype(F32)
    r = lax.broadcasted_iota(jnp.int32, (n_ep * big, bkeys), 0)
    k = lax.broadcasted_iota(jnp.int32, (n_ep * big, bkeys), 1)
    b = r // big
    s = r % slot
    dz = paired_vec(both_ways * (b // (both_ways * nx)) + b % both_ways, nz)
    dx = paired_vec((b % (both_ways * nx)) // both_ways, nx)
    dest = ((my_z + dz) & (nz - 1)) * nx + ((my_x + dx) & (nx - 1))
    slot_e = (dest * n_loc + s // CAP).astype(F32)
    same = ((r // slot) % nq) == (k // t_rows)
    hit0 = (slot_e == names[0:1, :]).astype(F32)
    hit1 = (slot_e == names[1:2, :]).astype(F32)
    before = jnp.dot(hit0 + hit1, tri, preferred_element_type=F32)
    taken = same & (before == (s % CAP).astype(F32))
    combine = jnp.where(taken, hit0 * names[2:3, :] + hit1 * names[3:4, :], 0.0).T
    pr = lax.broadcasted_iota(jnp.int32, (crow, crow), 0)
    pc = lax.broadcasted_iota(jnp.int32, (crow, crow), 1)
    perm = (
        ((pr // xrow) == ((pc // slot) % 2))
        & (((pr // slot) % per) == (pc // blk))
        & ((pr % slot) == (pc % slot))
    ).astype(BF16)
    xr = lax.broadcasted_iota(jnp.int32, (brow, xrow), 0)
    xc = lax.broadcasted_iota(jnp.int32, (brow, xrow), 1)
    expand = (((xr // big) == (xc // slot)) & ((xr % slot) == (xc % slot))).astype(BF16)
    sr = lax.broadcasted_iota(jnp.int32, (brow, 128), 0)
    sc = lax.broadcasted_iota(jnp.int32, (brow, 128), 1)
    in_lane = (sr % big) == sc
    gr = lax.broadcasted_iota(jnp.int32, (per, brow), 0)
    gc = lax.broadcasted_iota(jnp.int32, (per, brow), 1)
    in_block = gr == (gc // big)
    br = lax.broadcasted_iota(jnp.int32, (128, brow), 0)
    bc = lax.broadcasted_iota(jnp.int32, (128, brow), 1)
    unlane = (br == (bc % big)).astype(BF16)
    loads[9].wait()
    for g in range(CORES):
        for q in range(nq):
            for h in range(2):
                at = (CORES * (2 * q + h) + g) * part
                ed[g, q * hid : (q + 1) * hid, h * part : (h + 1) * part] = ednat[
                    :, at : at + part
                ]

    for c in order:
        at = pl.ds(c * per, per - (c == n_chunk - 1))
        remote(
            disp_send.at[at], grid.at[core, row, at], di_s, di_r.at[c], me, tp
        ).wait_recv()
        for d in far_rows:
            spot = grid.at[core, row, chunk(c)]
            remote(spot, spot, ya_s, ya_r.at[c], me, turn(row, d, n_row) * CORES + core).start()

    for i in (3, 4, 5):
        loads[i].wait()
    at = pl.ds(0, n_tp - 1)
    remote(tok.at[at], tok.at[at], ag_s, ag_r, me, tp).wait_recv()
    squares = jnp.zeros((t_rows, part), F32)
    for t in range(n_tp):
        x = tok[t].astype(F32)
        squares += x * x
    inv = lax.rsqrt(jnp.sum(squares, axis=1, keepdims=True) / width + norm_eps)
    mix = jnp.zeros((t_rows, part), F32)
    for t in range(n_tp):
        cols = slice(t * part, (t + 1) * part)
        nt = (tok[t].astype(F32) * inv * gain[:, cols]).astype(BF16)
        normed[:, cols] = nt
        mix += nt.astype(F32) * mixw[:, cols]
    mix_gate = 1.0 / (1.0 + jnp.exp(-jnp.sum(mix, axis=1, keepdims=True)))
    for i in (6, 7, 8):
        loads[i].wait()
    both = lax.dot_general(normed[...], wd[...], NT, preferred_element_type=F32)
    dh = (silu(both[:, 0:ffd]) * both[:, ffd : 2 * ffd]).astype(BF16)
    for t in range(n_tp):
        dense_send[t] = jnp.dot(
            dh, dd[:, t * part : (t + 1) * part], preferred_element_type=F32
        )
    for d in far_tp:
        t = turn(tp, d, n_tp)
        remote(dense_send.at[t], dense_recv.at[d - 1], de_s, de_r, me, t).start()
    for i in (10, 11):
        loads[i].wait()

    def unpack(c, g):
        slabs = [
            grid[g, y, c * per : (c + 1) * per].astype(F32).reshape(crow, half)
            for y in range(n_row)
        ]
        moved = jnp.dot(
            perm, jnp.concatenate(slabs, axis=1).astype(BF16), preferred_element_type=F32
        )
        total = jnp.zeros((xrow, half), F32)
        for y in range(n_row):
            for h in range(2):
                v = moved[h * xrow : (h + 1) * xrow, y * half : (y + 1) * half]
                at = pl.multiple_of((CORES * y + g) * part + h * half, half)
                rows_n[c * xrow : (c + 1) * xrow, pl.ds(at, half)] = v.astype(BF16)
                total += v * v
        return jnp.sum(total, axis=1, keepdims=True)

    ar = lax.broadcasted_iota(jnp.int32, (xrow, hid), 0)
    ac = lax.broadcasted_iota(jnp.int32, (xrow, hid), 1)
    mine = ((ar % slot) // CAP) == (ac // (hid // n_loc))
    hr = lax.broadcasted_iota(jnp.int32, (brow, hid), 0)
    seen = {}

    def gather(c):
        at = pl.ds(0, n_row - 1)
        spot = grid.at[core, at, chunk(c)]
        remote(spot, spot, ya_s, ya_r.at[c], me, tp).wait_recv()
        spot = grid.at[core, :, chunk(c)]
        remote(spot, spot, pf_s, pf_r.at[c], me, partner).start()
        seen[c] = unpack(c, core)

    def apply(c):
        spot = grid.at[1 - core, :, chunk(c)]
        remote(spot, spot, pf_s, pf_r.at[c], me, tp).wait_recv()
        inv = lax.rsqrt((seen[c] + unpack(c, 1 - core)) / width + norm_eps)
        rows = slice(c * xrow, (c + 1) * xrow)
        for t in range(n_tp):
            cols = slice(t * part, (t + 1) * part)
            rows_n[rows, cols] = (rows_n[rows, cols].astype(F32) * inv * gain[:, cols]).astype(
                BF16
            )
        act = lax.dot_general(rows_n[rows, :], wgu[...], NT, preferred_element_type=F32)
        hidden = jnp.where(mine, silu(act[:, 0:hid]) * act[:, hid : 2 * hid], 0.0)
        wider = jnp.dot(expand, hidden.astype(BF16), preferred_element_type=F32)
        rows = slice(c * brow, (c + 1) * brow)
        for q in range(nq):
            hid4[rows, q * hid : (q + 1) * hid] = jnp.where(
                ((hr // slot) % nq) == q, wider, 0.0
            ).astype(BF16)
        pair_send[rows, :] = jnp.dot(hid4[rows, :], ed[1 - core], preferred_element_type=F32)
        at = pl.ds(c * brow, brow)
        remote(pair_send.at[at], pair_recv.at[at], pa_s, pa_r.at[c], me, partner).start()

    def reply(c):
        rows = slice(c * brow, (c + 1) * brow)
        v = jnp.dot(hid4[rows, :], ed[core], preferred_element_type=F32)
        at = pl.ds(c * brow, brow)
        remote(pair_send.at[at], pair_recv.at[at], pa_s, pa_r.at[c], me, tp).wait_recv()
        v = v + pair_recv[rows, :]
        peak = jnp.max(jnp.abs(v), axis=1, keepdims=True)
        step = (jnp.maximum(peak, 1e-30) * (1.0 / 32600.0)).astype(BF16).astype(F32)
        lanes = jnp.where(in_lane, step, 0.0).astype(BF16)
        steps = jnp.dot(in_block.astype(BF16), lanes, preferred_element_type=F32)
        for i in range(per):
            j = c * per + i
            scl_send[j] = steps[i : i + 1, :]
            if j < n_ep - 1:
                remote(
                    scl_send.at[j], scl_recv.at[j], sc_s, sc_r.at[c], behind(j), tp
                ).start()
        ret_send[rows, :] = (
            jnp.floor(v * (1.0 / step) + 0.5).astype(jnp.int32).astype(jnp.int16)
        )
        for i in range(per):
            j = c * per + i
            if j < n_ep - 1:
                at = pl.ds(j * big, big)
                remote(
                    ret_send.at[at], ret_recv.at[at], re_s, re_r.at[c], behind(j), tp
                ).start()
        if c == n_chunk - 1:
            tail = slice((n_ep - 1) * big, n_ep * big)
            ret_recv[tail, :] = ret_send[tail, :]
            scl_recv[n_ep - 1] = scl_send[n_ep - 1]

    for run, i in (
        (gather, 0),
        (apply, 0),
        (gather, 1),
        (reply, 0),
        (apply, 1),
        (gather, 2),
        (reply, 1),
        (gather, 3),
        (apply, 2),
        (apply, 3),
        (reply, 2),
        (reply, 3),
    ):
        run(order[i])
    at = pl.ds(0, n_tp - 1)
    remote(dense_recv.at[at], dense_recv.at[at], de_s, de_r, me, tp).wait_recv()
    total = dense_send[tp]
    for d in range(1, n_tp):
        total += dense_recv[d - 1]
    total = mix_gate * total
    mixed = jnp.zeros((bkeys, wide), F32)
    for c in order:
        n = per - (c == n_chunk - 1)
        at = pl.ds(c * brow, n * big)
        remote(ret_send.at[at], ret_recv.at[at], re_s, re_r.at[c], me, tp).wait_recv()
        at = pl.ds(c * per, n)
        remote(scl_send.at[at], scl_recv.at[at], sc_s, sc_r.at[c], me, tp).wait_recv()
        rows = slice(c * brow, (c + 1) * brow)
        steps = jnp.concatenate([scl_recv[c * per + i] for i in range(per)], axis=0)
        lanes = jnp.dot(steps.astype(BF16), unlane, preferred_element_type=F32)
        step = jnp.sum(jnp.where(in_block, lanes, 0.0), axis=0, keepdims=True)
        back = ret_recv[rows, :].astype(jnp.int32).astype(F32)
        mixed += jnp.dot(
            combine[:, rows] * step,
            back,
            preferred_element_type=F32,
            precision=lax.Precision.HIGHEST,
        )
    for q in range(nq):
        for h in range(2):
            fin_send[2 * q + h] = mixed[
                q * t_rows : (q + 1) * t_rows, h * part : (h + 1) * part
            ]
    for d in far_rows:
        y = turn(row, d, n_row)
        remote(
            fin_send.at[y], fin_recv.at[d - 1], fi_s, fi_r, me, y * CORES + core
        ).start()
    remote(fin_recv, fin_recv, fi_s, fi_r, me, tp).wait_recv()
    total += fin_send[row]
    for d in range(1, n_row):
        total += fin_recv[d - 1]
    eye = lax.broadcasted_iota(jnp.int32, (t_rows, 128), 0) == lax.broadcasted_iota(
        jnp.int32, (t_rows, 128), 1
    )
    mine_sq = jnp.sum(
        jnp.where(eye, jnp.sum(total * total, axis=1, keepdims=True), 0.0),
        axis=0,
        keepdims=True,
    )
    sq_send[...] = mine_sq
    for d in far_tp:
        remote(sq_send, sq_recv.at[d - 1], sq_s, sq_r, me, turn(tp, d, n_tp)).start()
    remote(sq_recv, sq_recv, sq_s, sq_r, me, tp).wait_recv()
    all_sq = mine_sq
    for d in range(1, n_tp):
        all_sq += sq_recv[d - 1]
    all_sq = jnp.sum(jnp.where(eye, all_sq, 0.0), axis=1, keepdims=True)
    scale = lax.rsqrt(all_sq / width + norm_eps)
    out_ref[...] = (total * scale * og[...]).astype(out_ref.dtype)
    at = pl.ds(0, n_tp - 1)
    remote(tok.at[at], tok.at[at], ag_s, ag_r, me, tp).wait_send()
    remote(dense_recv.at[at], dense_recv.at[at], de_s, de_r, me, tp).wait_send()
    remote(sq_recv, sq_recv, sq_s, sq_r, me, tp).wait_send()
    at = pl.ds(0, n_ep - 1)
    remote(disp_send.at[at], disp_send.at[at], di_s, di_r.at[0], me, tp).wait_send()
    remote(scl_send.at[at], scl_recv.at[at], sc_s, sc_r.at[0], me, tp).wait_send()
    at = pl.ds(0, (n_ep - 1) * big)
    remote(ret_send.at[at], ret_recv.at[at], re_s, re_r.at[0], me, tp).wait_send()
    spot = grid.at[0, pl.ds(0, n_row - 1)]
    remote(spot, spot, ya_s, ya_r.at[0], me, tp).wait_send()
    remote(grid.at[0], grid.at[0], pf_s, pf_r.at[0], me, tp).wait_send()
    remote(pair_send, pair_recv, pa_s, pa_r.at[0], me, tp).wait_send()
    remote(fin_recv, fin_recv, fi_s, fi_r, me, tp).wait_send()


def shards(n_ep, n_tp, *args):
    (tok, gain, route, logit, eg, eu, ed, dg, du, dd, mixw, og) = args
    t_rows, part = tok.shape
    width = part * n_tp
    half = part // 2
    n_loc, _, ff = eg.shape
    ffd = dg.shape[1]
    hid = n_loc * ff
    n_row = n_tp // CORES
    slot = n_loc * CAP
    blk = 2 * slot
    nq = n_row // 2
    big = n_ep * nq * slot
    wide = 2 * part
    n_chunk = chunks_of(n_ep)
    dma = pltpu.SemaphoreType.DMA
    V = pltpu.VMEM
    scratch = [
        V((n_tp, t_rows, part), BF16),
        V((1, width), F32),
        V(route.shape[::-1], jnp.int32),
        V(logit.shape[::-1], F32),
        V((2 * hid, width), BF16),
        V((hid, width), BF16),
        V((CORES, nq * hid, wide), BF16),
        V((2 * ffd, width), BF16),
        V(dd.shape, BF16),
        V((1, width), F32),
        V((1, part), F32),
        V((t_rows, width), BF16),
        V((n_ep, blk, half), BF16),
        V((CORES, n_row, n_ep, blk, half), BF16),
        V((n_ep * slot, width), BF16),
        V((big, nq * hid), BF16),
        V((n_tp, t_rows, part), F32),
        V((n_tp - 1, t_rows, part), F32),
        V((big, wide), F32),
        V((big, wide), F32),
        V((big, wide), jnp.int16),
        V((big, wide), jnp.int16),
        V((n_ep, 1, 128), F32),
        V((n_ep, 1, 128), F32),
        V((n_row, t_rows, part), F32),
        V((n_row - 1, t_rows, part), F32),
        V((1, 128), F32),
        V((n_tp - 1, 1, 128), F32),
        dma((12,)),
        dma,
        dma,
        dma,
        dma((n_chunk,)),
        dma,
        dma((n_chunk,)),
        dma,
        dma((n_chunk,)),
        dma,
        dma,
        dma,
        dma((n_chunk,)),
        dma,
        dma((n_chunk,)),
        dma,
        dma((n_chunk,)),
        dma,
        dma,
        dma,
        dma,
    ]
    return pl.pallas_call(
        functools.partial(kernel, n_ep, n_tp, n_loc),
        out_shape=jax.ShapeDtypeStruct((t_rows, part), BF16),
        in_specs=[pl.BlockSpec(memory_space=pltpu.HBM)] * 12,
        out_specs=pl.BlockSpec(memory_space=pltpu.VMEM),
        scratch_shapes=scratch,
        compiler_params=pltpu.CompilerParams(
            collective_id=0, has_side_effects=True, vmem_limit_bytes=60 * 1024 * 1024
        ),
        name="moe_layer",
    )(
        tok,
        gain.reshape(1, width),
        route.T,
        logit.T,
        eg.swapaxes(1, 2).reshape(hid, width),
        eu.swapaxes(1, 2).reshape(hid, width),
        ed.reshape(hid, width),
        dg.T,
        du.T,
        dd,
        mixw.reshape(1, width),
        og.reshape(1, part),
    )


def solution(mesh):
    placed = (
        P("ep", "tp"),
        P(),
        P("ep", None),
        P("ep", None),
        P("ep", None, "tp"),
        P("ep", None, "tp"),
        P("ep", "tp", None),
        P(None, "tp"),
        P(None, "tp"),
        P("tp", None),
        P(),
        P("tp"),
    )
    return jax.shard_map(
        functools.partial(shards, mesh.shape["ep"], mesh.shape["tp"]),
        mesh=mesh,
        in_specs=placed,
        out_specs=P("ep", "tp"),
        check_vma=False,
    )
```
